128 devices in a mesh: fs: 16 (over z, x), tp: 8 (over y, core).
Axes of the slice: x: 4, y: 4, z: 4, core: 2. Of those that a mesh axis runs over, the one named last changes fastest.
Arguments:
- tokens: bfloat16 [16384, 2048], P(('fs', 'tp')), may hold values from -6 to 6
- mix_gain: float32 [2048], replicated, may hold values from 0.1 to 1.9
- ffn_gain: float32 [2048], replicated, may hold values from 0.1 to 1.9
- u_weight: float32 [2048, 2048], P('fs', 'tp'), may hold values from -0.125 to 0.125
- u_scale: float32 [2048], P('tp'), may hold values from 0.5 to 2
- v_weight: float32 [2048, 2048], P('fs', 'tp'), may hold values from -0.125 to 0.125
- v_scale: float32 [2048], P('tp'), may hold values from 0.3 to 12
- v_gain: float32 [2048], P('tp'), may hold values from 0.1 to 1.9
- spatial_weight: bfloat16 [8, 128, 128], replicated, may hold values from -0.5 to 0.5
- spatial_bias: float32 [8, 128], replicated, may hold values from 0.1 to 1.9
- out_weight: float32 [2048, 2048], P('tp', 'fs'), may hold values from -0.125 to 0.125
- out_scale: float32 [2048], P('fs'), may hold values from 0.5 to 2
- gate_weight: float32 [2048, 6144], P('fs', 'tp'), may hold values from -0.125 to 0.125
- gate_scale: float32 [6144], P('tp'), may hold values from 0.5 to 2
- up_weight: float32 [2048, 6144], P('fs', 'tp'), may hold values from -0.125 to 0.125
- up_scale: float32 [6144], P('tp'), may hold values from 0.5 to 2
- down_weight: float32 [6144, 2048], P('tp', 'fs'), may hold values from -0.078125 to 0.078125
- down_scale: float32 [2048], P('fs'), may hold values from 0.5 to 2
Outputs:
- layer_out: bfloat16 [16384, 2048], P(('fs', 'tp'))
The draws below stay inside these ranges and needn't reach their ends.
All inputs are finite; a program needn't handle non-finite values.
Results may differ from the reference program's by a relative error of at most 0.02.
Values may be sent and summed in bfloat16 or wider, within the bound.
A program may use at most 64 MiB of HBM per device.

```python
import math
import jax
import jax.numpy as jnp
from jax import lax

D = 2048
A = 2048
A_GROUPS = 8
BLK = 128
FF = 6144
TOKENS = 16384
N_TP = 8


def draw_v_scale(key, part):
    column_ramp = jnp.arange(A, dtype=jnp.float32) / A
    base_scale = jnp.exp(jax.random.uniform(key, (A,), jnp.float32, math.log(0.3), math.log(3.0)))
    return base_scale * 3.0 ** column_ramp


def block_levels(key, dims, split, low, largest):
    loudness, own = 1.0, jax.random.fold_in(key, 6)
    for dim, parts in split:
        heights = jnp.exp(jax.random.uniform(jax.random.fold_in(own, dim), (parts,), jnp.float32, low / len(split), largest / len(split)))
        loudness = loudness * jnp.repeat(heights, dims[dim] // parts).reshape([-1 if axis == dim else 1 for axis in range(len(dims))])
    return loudness


def centred(rng, dims, scale, reach, pieces=(), held_as=jnp.bfloat16):
    factor_of = block_levels(rng, dims, pieces, -0.22, 0.18) if pieces else 1.0
    entries = jax.random.normal(rng, dims, jnp.float32) * scale * factor_of
    return jnp.minimum(jnp.maximum(entries, -reach), reach).astype(held_as)


def setup_inputs(seed: int = 0) -> dict:
    keys = jax.random.split(jax.random.key(seed), 19)
    tokens = centred(keys[0], (TOKENS, D), 1.0, 6.0, ((0, 128),))
    mix_gain = jnp.clip(1.0 + 0.18 * jax.random.normal(keys[1], (D,), jnp.float32), 0.1, 1.9)
    ffn_gain = jnp.clip(1.0 + 0.18 * jax.random.normal(keys[2], (D,), jnp.float32), 0.1, 1.9)
    u_weight = centred(keys[3], (D, A), D ** -0.5, 0.125, ((0, 16), (1, 8)), jnp.float32)
    u_scale = jnp.clip(jnp.exp(math.log(2.0) - 1.3862944 * jax.random.uniform(keys[4], (A,), jnp.float32) ** block_levels(keys[4], (A,), ((0, 8),), -0.2, 0.2)), 0.5, 2.0)
    v_weight = centred(keys[5], (D, A), D ** -0.5, 0.125, ((0, 16), (1, 8)), jnp.float32)
    v_scale = draw_v_scale(jax.random.fold_in(keys[18], 71), 0)
    v_gain = jnp.clip(1.0 + 0.18 * jax.random.normal(keys[7], (A,), jnp.float32), 0.1, 1.9)
    spatial_weight = centred(keys[8], (A_GROUPS, BLK, BLK), BLK ** -0.5, 0.5)
    spatial_bias = jnp.clip(1.0 + 0.18 * jax.random.normal(keys[9], (A_GROUPS, BLK), jnp.float32), 0.1, 1.9)
    out_weight = centred(keys[10], (A, D), A ** -0.5, 0.125, ((0, 8), (1, 16)), jnp.float32)
    out_scale = jnp.clip(jnp.exp(math.log(2.0) - 1.3862944 * jax.random.uniform(keys[11], (D,), jnp.float32) ** block_levels(keys[11], (D,), ((0, 16),), -0.2, 0.2)), 0.5, 2.0)
    gate_weight = centred(keys[12], (D, FF), D ** -0.5, 0.125, ((0, 16), (1, 8)), jnp.float32)
    gate_scale = jnp.clip(jnp.exp(math.log(2.0) - 1.3862944 * jax.random.uniform(keys[13], (FF,), jnp.float32) ** block_levels(keys[13], (FF,), ((0, 8),), -0.2, 0.2)), 0.5, 2.0)
    up_weight = centred(keys[14], (D, FF), D ** -0.5, 0.125, ((0, 16), (1, 8)), jnp.float32)
    up_scale = jnp.clip(jnp.exp(math.log(2.0) - 1.3862944 * jax.random.uniform(keys[15], (FF,), jnp.float32) ** block_levels(keys[15], (FF,), ((0, 8),), -0.2, 0.2)), 0.5, 2.0)
    down_weight = centred(keys[16], (FF, D), FF ** -0.5, 0.078125, ((0, 8), (1, 16)), jnp.float32)
    down_scale = jnp.clip(jnp.exp(math.log(2.0) - 1.3862944 * jax.random.uniform(keys[17], (D,), jnp.float32) ** block_levels(keys[17], (D,), ((0, 16),), -0.2, 0.2)), 0.5, 2.0)
    return {"tokens": tokens, "mix_gain": mix_gain, "ffn_gain": ffn_gain, "u_weight": u_weight, "u_scale": u_scale, "v_weight": v_weight, "v_scale": v_scale, "v_gain": v_gain, "spatial_weight": spatial_weight, "spatial_bias": spatial_bias, "out_weight": out_weight, "out_scale": out_scale, "gate_weight": gate_weight, "gate_scale": gate_scale, "up_weight": up_weight, "up_scale": up_scale, "down_weight": down_weight, "down_scale": down_scale}


def rms_rows(values, norm_gain):
    widened = values.astype(jnp.float32)
    factor = lax.rsqrt(lax.optimization_barrier(jnp.mean(widened * widened, axis=1, keepdims=True)) + 1e-06)
    return (widened * factor * norm_gain).astype(jnp.bfloat16)

def project(values, matrix, scales):
    return jnp.dot(values, matrix.astype(jnp.bfloat16), preferred_element_type=jnp.float32) * scales

def run_sums(values, matrix, scales):
    run_length = values.shape[1] // N_TP
    narrow = matrix.astype(jnp.bfloat16)
    summed = jnp.zeros((values.shape[0], matrix.shape[1]), jnp.float32)
    for run_index in range(N_TP):
        lower = run_index * run_length
        partial_value = jnp.dot(values[:, lower:lower + run_length], narrow[lower:lower + run_length], preferred_element_type=jnp.float32) * scales
        summed = summed + lax.optimization_barrier(partial_value.astype(jnp.bfloat16)).astype(jnp.float32)
    return summed

def reference(tokens, mix_gain, ffn_gain, u_weight, u_scale, v_weight, v_scale, v_gain, spatial_weight, spatial_bias, out_weight, out_scale, gate_weight, gate_scale, up_weight, up_scale, down_weight, down_scale):
    normed = rms_rows(tokens, mix_gain)
    u_values = jax.nn.gelu(project(normed, u_weight, u_scale), approximate=True).astype(jnp.bfloat16)
    v_values = jax.nn.gelu(project(normed, v_weight, v_scale), approximate=True).astype(jnp.bfloat16)
    v_wide = v_values.astype(jnp.float32)
    average = lax.optimization_barrier(jnp.mean(v_wide, axis=1, keepdims=True))
    spread = lax.optimization_barrier(jnp.mean(v_wide * v_wide, axis=1, keepdims=True)) - average * average
    v_normed = ((v_wide - average) * lax.rsqrt(spread + 1e-05) * v_gain).astype(jnp.bfloat16)
    group_dim = A // A_GROUPS
    blocks = v_normed.reshape(TOKENS // BLK, BLK, A_GROUPS, group_dim).astype(jnp.float32)
    causal = jnp.tril(jnp.ones((BLK, BLK), dtype=bool))
    masked = jnp.where(causal[None], spatial_weight, jnp.zeros_like(spatial_weight)).astype(jnp.float32)
    mixed_sum = jnp.einsum('gts,bsgd->btgd', masked, blocks) + spatial_bias.T[None, :, :, None]
    gated_rows = (u_values.reshape(blocks.shape).astype(jnp.float32) * mixed_sum).astype(jnp.bfloat16)
    gated_rows = gated_rows.reshape(TOKENS, A)
    residual = (tokens.astype(jnp.float32) + run_sums(gated_rows, out_weight, out_scale)).astype(jnp.bfloat16)
    normed_second = rms_rows(residual, ffn_gain)
    hidden = (jax.nn.silu(project(normed_second, gate_weight, gate_scale)) * project(normed_second, up_weight, up_scale)).astype(jnp.bfloat16)
    return (residual.astype(jnp.float32) + run_sums(hidden, down_weight, down_scale)).astype(jnp.bfloat16)
```

```python
import functools

import jax
import jax.numpy as jnp
from jax import lax
from jax.experimental import pallas as pl
from jax.experimental.pallas import tpu as pltpu
from jax.sharding import PartitionSpec as P

MESH = pl.DeviceIdType.MESH
F32 = jnp.float32
BF16 = jnp.bfloat16
A = 2048
BLK = 128
LEFT, RIGHT, OPP, OWN = 0, 1, 2, 3


def rms_rows(widened, norm_gain):
    factor = lax.rsqrt(jnp.mean(widened * widened, axis=1, keepdims=True) + 1e-06)
    return (widened * factor * norm_gain).astype(BF16)


def gelu(x):
    return 0.5 * x * (1.0 + jnp.tanh(0.7978845608028654 * (x + 0.044715 * (x * x * x))))


def silu(x):
    return 0.5 * x * (1.0 + jnp.tanh(0.5 * x))


class Sends:
    def __init__(self, sems):
        self.sems, self.started = sems, []

    def start(self, src, dst, recv_sem, device):
        copy = pltpu.make_async_remote_copy(
            src_ref=src,
            dst_ref=dst,
            send_sem=self.sems.at[len(self.started)],
            recv_sem=recv_sem,
            device_id=device,
            device_id_type=MESH,
        )
        copy.start()
        self.started.append(copy)

    def finish(self):
        for copy in self.started:
            copy.wait_send()


def arrived(ref, sem, device):
    pltpu.make_async_remote_copy(
        src_ref=ref,
        dst_ref=ref,
        send_sem=sem,
        recv_sem=sem,
        device_id=device,
        device_id_type=MESH,
    ).wait_recv()


class Gather:
    def __init__(self, buf, sems, sends, place, x_first):
        self.buf, self.sems, self.sends, self.place, self.x_first = buf, sems, sends, place, x_first

    def peer(self, first, step):
        pc = self.place
        along_x = first == self.x_first
        x = lax.rem(pc["x"] + step + 4, 4) if along_x else pc["x"]
        z = pc["z"] if along_x else lax.rem(pc["z"] + step + 4, 4)
        return (z * 4 + x, pc["y"] * 2 + pc["c"])

    def block(self, step, rows=None):
        pc = self.place
        x = lax.rem(pc["x"] + step + 4, 4) if self.x_first else pc["x"]
        z = pc["z"] if self.x_first else lax.rem(pc["z"] + step + 4, 4)
        ref = self.buf.at[pc["c"], z, x]
        return ref if rows is None else ref.at[rows]

    def group(self, step, half=None, core=None):
        pc = self.place
        core = pc["c"] if core is None else core
        part = slice(None) if half is None else pl.ds(2 * half, 2)
        if self.x_first:
            return self.buf.at[core, lax.rem(pc["z"] + step + 4, 4), part]
        return self.buf.at[core, part, lax.rem(pc["x"] + step + 4, 4)]

    def halves(self):
        rows = self.buf.shape[3] // 2
        return pl.ds(0, rows), pl.ds(rows, rows)

    def send(self, src, slot, device):
        self.sends.start(src, src, self.sems.at[slot], device)

    def share(self, ref, slot):
        self.send(ref, slot, self.place["partner"])

    def wait(self, ref, slot):
        arrived(ref, self.sems.at[slot], self.place["partner"])

    def first_start(self):
        self.send(self.block(0), 0, self.peer(True, 1))
        self.send(self.block(0), 1, self.peer(True, -1))

    def first_relay(self):
        low, high = self.halves()
        self.wait(self.block(-1), 0)
        self.send(self.block(-1, low), 2, self.peer(True, 1))
        self.wait(self.block(1), 1)
        self.send(self.block(1, high), 3, self.peer(True, -1))

    def second_start(self):
        low, high = self.halves()
        self.wait(self.block(2, low), 2)
        self.wait(self.block(2, high), 3)
        self.send(self.group(0), 4, self.peer(False, 1))
        self.send(self.group(0), 5, self.peer(False, -1))
        self.share(self.group(0), 8)

    def second_relay(self):
        self.wait(self.group(-1), 4)
        self.send(self.group(-1, 0), 6, self.peer(False, 1))
        self.share(self.group(-1), 9)
        self.wait(self.group(1), 5)
        self.send(self.group(1, 1), 7, self.peer(False, -1))
        self.share(self.group(1), 10)

    def second_end(self):
        self.wait(self.group(2, 0), 6)
        self.share(self.group(2, 0), 11)
        self.wait(self.group(2, 1), 7)
        self.share(self.group(2, 1), 12)

    def from_partner(self):
        other = 1 - self.place["c"]
        self.wait(self.group(0, core=other), 8)
        self.wait(self.group(-1, core=other), 9)
        self.wait(self.group(1, core=other), 10)
        self.wait(self.group(2, 0, other), 11)
        self.wait(self.group(2, 1, other), 12)


N_GATHER_SEMS = 13
N_SENDS = 160


def layer_kernel(
    tok_hbm, u_hbm, v_hbm, o_hbm, g_hbm, p_hbm, d_hbm,
    mix_gain, ffn_gain, u_scale, v_scale, v_gain, o_scale, g_scale, p_scale, d_scale,
    spatial, bias, out_ref,
    tok, u32, v32, o32, g32, p32, d32,
    ub, vb, oab, obb, gb, pb, dab, dbb,
    x1, x2, u_val, v_val, gated, hid, part1, part2, relay1, relay2, fl1, fr1, fl2, fr2, res,
    stat, stat_in, vg,
    load_sems, send_sems, gather_sems, tok_sems, misc_sems,
):
    fs = lax.axis_index("fs")
    tp = lax.axis_index("tp")
    z, x = fs // 4, lax.rem(fs, 4)
    y, c = tp // 2, lax.rem(tp, 2)
    partner = (fs, y * 2 + (1 - c))
    y_right = (fs, lax.rem(y + 1, 4) * 2 + c)
    y_left = (fs, lax.rem(y + 3, 4) * 2 + c)
    y_opp = (fs, lax.rem(y + 2, 4) * 2 + c)
    place = {"x": x, "y": y, "z": z, "c": c, "partner": partner}

    loads = []
    for n, (src, dst) in enumerate(
        ((tok_hbm, tok), (u_hbm, u32), (v_hbm, v32), (o_hbm, o32), (g_hbm, g32), (p_hbm, p32), (d_hbm, d32))
    ):
        copy = pltpu.make_async_copy(src, dst, load_sems.at[n])
        copy.start()
        loads.append(copy)

    barrier = pltpu.get_barrier_semaphore()
    plane = [
        (z * 4 + lax.rem(x + 1, 4), tp),
        (z * 4 + lax.rem(x + 3, 4), tp),
        (lax.rem(z + 1, 4) * 4 + x, tp),
        (lax.rem(z + 3, 4) * 4 + x, tp),
    ]
    peers = [partner, y_right, y_left, y_opp] + plane
    for peer in peers:
        pl.semaphore_signal(barrier, inc=1, device_id=peer, device_id_type=MESH)

    sends = Sends(send_sems)
    gather = [
        Gather(buf, gather_sems.at[n], sends, place, n % 2 == 0)
        for n, buf in enumerate((ub, vb, oab, obb, gb, pb, dab, dbb))
    ]
    gu, gv, goa, gob, gg, gp, gda, gdb = gather
    uv, outs, ffn, downs = (gu, gv), (goa, gob), (gg, gp), (gda, gdb)

    loads[1].wait()
    ub[c, z, x] = (u32[...] * u_scale[...]).astype(BF16)
    loads[2].wait()
    vb[c, z, x] = (v32[...] * v_scale[...]).astype(BF16)
    loads[3].wait()
    half = o32.shape[0] // 2
    oab[c, z, x] = (o32[:half] * o_scale[...]).astype(BF16)
    obb[c, z, x] = (o32[half:] * o_scale[...]).astype(BF16)
    vg[c] = jnp.broadcast_to(v_gain[...], vg.shape[1:])
    loads[0].wait()
    x1[OWN] = rms_rows(tok[...].astype(F32), mix_gain[...])

    pl.semaphore_wait(barrier, len(peers))

    H0, H1 = pl.ds(0, 64), pl.ds(64, 64)

    def rows_start(buf, base):
        sends.start(buf.at[OWN, H0], buf.at[LEFT, H0], tok_sems.at[base + 0], y_right)
        sends.start(buf.at[OWN, H1], buf.at[RIGHT, H1], tok_sems.at[base + 1], y_left)
        sends.start(buf.at[OWN, H1], buf.at[LEFT, H1], tok_sems.at[base + 2], y_right)
        sends.start(buf.at[OWN, H0], buf.at[RIGHT, H0], tok_sems.at[base + 3], y_left)

    def rows_relay(buf, base):
        arrived(buf.at[LEFT, H0], tok_sems.at[base + 0], y_left)
        sends.start(buf.at[LEFT, H0], buf.at[OPP, H0], tok_sems.at[base + 4], y_right)
        arrived(buf.at[RIGHT, H1], tok_sems.at[base + 1], y_right)
        sends.start(buf.at[RIGHT, H1], buf.at[OPP, H1], tok_sems.at[base + 5], y_left)

    def rows_near(buf, base):
        arrived(buf.at[LEFT, H1], tok_sems.at[base + 2], y_left)
        arrived(buf.at[RIGHT, H0], tok_sems.at[base + 3], y_right)

    def rows_far(buf, base):
        arrived(buf.at[OPP, H0], tok_sems.at[base + 4], y_left)
        arrived(buf.at[OPP, H1], tok_sems.at[base + 5], y_right)

    def sums_far(part, relay, base):
        sends.start(part.at[OPP, H0], relay.at[0], tok_sems.at[base + 0], y_right)
        sends.start(part.at[OPP, H1], relay.at[1], tok_sems.at[base + 1], y_left)

    def sums_near(part, fl, fr, base):
        sends.start(part.at[RIGHT, H1], fl.at[H1], tok_sems.at[base + 2], y_right)
        sends.start(part.at[LEFT, H0], fr.at[H0], tok_sems.at[base + 3], y_left)

    def sums_relay(part, relay, fl, fr, base):
        arrived(relay.at[0], tok_sems.at[base + 0], y_left)
        part[RIGHT, H0] = (part[RIGHT, H0].astype(F32) + relay[0].astype(F32)).astype(BF16)
        sends.start(part.at[RIGHT, H0], fl.at[H0], tok_sems.at[base + 4], y_right)
        arrived(relay.at[1], tok_sems.at[base + 1], y_right)
        part[LEFT, H1] = (part[LEFT, H1].astype(F32) + relay[1].astype(F32)).astype(BF16)
        sends.start(part.at[LEFT, H1], fr.at[H1], tok_sems.at[base + 5], y_left)

    def sums_end(fl, fr, base):
        arrived(fl.at[H1], tok_sems.at[base + 2], y_left)
        arrived(fr.at[H0], tok_sems.at[base + 3], y_right)
        arrived(fl.at[H0], tok_sems.at[base + 4], y_left)
        arrived(fr.at[H1], tok_sems.at[base + 5], y_right)

    for g in uv:
        g.first_start()
    rows_start(x1, 0)
    for g in outs:
        g.first_start()
    sends.start(vg.at[c], vg.at[c], misc_sems.at[3], partner)

    loads[4].wait()
    gb[c, z, x] = (g32[...] * g_scale[...]).astype(BF16)
    loads[5].wait()
    pb[c, z, x] = (p32[...] * p_scale[...]).astype(BF16)
    loads[6].wait()
    half = d32.shape[0] // 2
    dab[c, z, x] = (d32[:half] * d_scale[...]).astype(BF16)
    dbb[c, z, x] = (d32[half:] * d_scale[...]).astype(BF16)

    for g in uv:
        g.first_relay()
    for g in outs:
        g.first_relay()
    for g in uv:
        g.second_start()
    rows_relay(x1, 0)
    for g in uv:
        g.second_relay()
    for g in outs:
        g.second_start()
    for g in ffn:
        g.first_start()
    for g in uv:
        g.second_end()
    rows_near(x1, 0)
    rows_far(x1, 0)
    for g in outs:
        g.second_relay()
    for g in uv:
        g.from_partner()

    slot_chip = [lax.rem(y + 3, 4), lax.rem(y + 1, 4), lax.rem(y + 2, 4), y]
    row_ids = lax.broadcasted_iota(jnp.int32, (BLK, BLK), 0)
    col_ids = lax.broadcasted_iota(jnp.int32, (BLK, BLK), 1)
    eye = row_ids == col_ids
    stat[...] = jnp.zeros_like(stat)

    def project_mixer(first):
        rows = x1[first : first + 2].reshape(2 * BLK, -1)
        sums = squares = None
        for core in range(2):
            cols = slice(core * 256, core * 256 + 256)
            u = gelu(jnp.dot(rows, ub[core].reshape(A, 256), preferred_element_type=F32))
            v = gelu(jnp.dot(rows, vb[core].reshape(A, 256), preferred_element_type=F32)).astype(BF16)
            u_val[first : first + 2, :, cols] = u.astype(BF16).reshape(2, BLK, 256)
            v_val[first : first + 2, :, cols] = v.reshape(2, BLK, 256)
            wide = v.astype(F32)
            s, q = jnp.sum(wide, axis=1, keepdims=True), jnp.sum(wide * wide, axis=1, keepdims=True)
            sums, squares = (s, q) if core == 0 else (sums + s, squares + q)
        for k in range(2):
            for row, column in ((0, sums), (1, squares)):
                piece = column[k * BLK : (k + 1) * BLK]
                stat[slot_chip[first + k], row : row + 1, :] = jnp.sum(
                    jnp.where(eye, piece, 0.0), axis=0, keepdims=True
                )

    project_mixer(LEFT)
    for g in ffn:
        g.first_relay()
    project_mixer(OPP)
    sends.start(stat, stat_in.at[0], misc_sems.at[0], y_right)
    sends.start(stat, stat_in.at[1], misc_sems.at[1], y_left)
    sends.start(stat, stat_in.at[2], misc_sems.at[2], y_opp)
    for g in outs:
        g.second_end()
    for g in ffn:
        g.second_start()
    for g in downs:
        g.first_start()
    arrived(vg.at[1 - c], misc_sems.at[3], partner)
    arrived(stat_in.at[0], misc_sems.at[0], y_left)
    arrived(stat_in.at[1], misc_sems.at[1], y_right)
    arrived(stat_in.at[2], misc_sems.at[2], y_opp)

    mixers = []
    for core in range(2):
        masked = jnp.where(col_ids <= row_ids, spatial[2 * y + core].astype(F32), 0.0)
        offset = jnp.sum(jnp.where(eye, bias[2 * y + core], 0.0), axis=1, keepdims=True)
        mixers.append((masked, offset))

    def mix(slot):
        chip = slot_chip[slot]
        total = stat[chip] + stat_in[0, chip] + stat_in[1, chip] + stat_in[2, chip]
        average = total[0:1] * (1.0 / A)
        spread = total[1:2] * (1.0 / A) - average * average
        factor = lax.rsqrt(spread + 1e-05)
        for core in range(2):
            cols = slice(core * 256, core * 256 + 256)
            masked, offset = mixers[core]
            scaled = (masked * factor).astype(BF16)
            shift = jnp.sum(scaled.astype(F32) * average, axis=1, keepdims=True)
            mixed = jnp.dot(scaled, v_val[slot, :, cols], preferred_element_type=F32)
            mixed = (mixed - shift) * vg[core, 0:1, :] + offset
            gated[slot, :, cols] = (u_val[slot, :, cols].astype(F32) * mixed).astype(BF16)

    def project_out(first):
        @pl.loop(0, 8)
        def _(j):
            fz, fx = j // 2, lax.rem(j, 2) * 2
            total = None
            for core in range(2):
                matrix = jnp.concatenate(
                    [
                        jnp.concatenate([oab[core, fz, fx], obb[core, fz, fx]], axis=0),
                        jnp.concatenate([oab[core, fz, fx + 1], obb[core, fz, fx + 1]], axis=0),
                    ],
                    axis=1,
                )
                rows = gated[first : first + 2, :, core * 256 : core * 256 + 256].reshape(2 * BLK, 256)
                term = jnp.dot(rows, matrix, preferred_element_type=F32)
                total = term if core == 0 else total + term
            cols = pl.ds(pl.multiple_of(j * 256, 256), 256)
            part1[first : first + 2, :, cols] = total.astype(BF16).reshape(2, BLK, 256)

    mix(OPP)
    mix(OWN)
    for g in outs:
        g.from_partner()
    project_out(OPP)
    sums_far(part1, relay1, 6)
    mix(LEFT)
    mix(RIGHT)
    project_out(LEFT)
    sums_near(part1, fl1, fr1, 6)
    sums_relay(part1, relay1, fl1, fr1, 6)
    for g in downs:
        g.first_relay()
    sums_end(fl1, fr1, 6)
    total = tok[...].astype(F32) + part1[OWN].astype(F32)
    residual = (total + fl1[...].astype(F32) + fr1[...].astype(F32)).astype(BF16)
    res[...] = residual
    x2[OWN] = rms_rows(residual.astype(F32), ffn_gain[...])
    rows_start(x2, 12)
    for g in ffn:
        g.second_relay()
    rows_relay(x2, 12)
    for g in downs:
        g.second_start()
    for g in ffn:
        g.second_end()
    rows_near(x2, 12)
    for g in ffn:
        g.from_partner()

    def project_ffn(first):
        @pl.loop(0, 2)
        def _(core):
            for j in range(3):
                cols = slice(j * 256, j * 256 + 256)
                rows = x2[first : first + 2].reshape(2 * BLK, -1)
                gate = jnp.dot(rows, gb[core, :, :, :, cols].reshape(A, 256), preferred_element_type=F32)
                up = jnp.dot(rows, pb[core, :, :, :, cols].reshape(A, 256), preferred_element_type=F32)
                hid[core, :, cols] = (silu(gate) * up).astype(BF16)

    def project_down(first):
        @pl.loop(0, 8)
        def _(j):
            fz, fx = j // 2, lax.rem(j, 2) * 2
            total = None
            for core in range(2):
                matrix = jnp.concatenate(
                    [
                        jnp.concatenate([dab[core, fz, fx], dbb[core, fz, fx]], axis=0),
                        jnp.concatenate([dab[core, fz, fx + 1], dbb[core, fz, fx + 1]], axis=0),
                    ],
                    axis=1,
                )
                term = jnp.dot(hid[core], matrix, preferred_element_type=F32)
                total = term if core == 0 else total + term
            cols = pl.ds(pl.multiple_of(j * 256, 256), 256)
            part2[first : first + 2, :, cols] = total.astype(BF16).reshape(2, BLK, 256)

    project_ffn(LEFT)
    for g in downs:
        g.second_relay()
    for g in downs:
        g.second_end()
    for g in downs:
        g.from_partner()
    project_down(LEFT)
    sums_near(part2, fl2, fr2, 18)
    rows_far(x2, 12)
    project_ffn(OPP)
    project_down(OPP)
    sums_far(part2, relay2, 18)
    sums_relay(part2, relay2, fl2, fr2, 18)
    sums_end(fl2, fr2, 18)
    total = res[...].astype(F32) + part2[OWN].astype(F32)
    out_ref[...] = (total + fl2[...].astype(F32) + fr2[...].astype(F32)).astype(BF16)
    sends.finish()


def local(
    tokens, mix_gain, ffn_gain, u_weight, u_scale, v_weight, v_scale, v_gain, spatial_weight, spatial_bias,
    out_weight, out_scale, gate_weight, gate_scale, up_weight, up_scale, down_weight, down_scale,
):
    rows, width = tokens.shape
    row = lambda a: a.reshape(1, -1)
    bias = spatial_bias.reshape(spatial_bias.shape[0], 1, BLK)
    depth = u_weight.shape[0]
    ff = gate_weight.shape[1]
    mix_cols = u_weight.shape[1]
    out_cols = out_weight.shape[1]
    vm = pltpu.VMEM
    anywhere = pl.BlockSpec(memory_space=pl.ANY)
    on_chip = pl.BlockSpec(memory_space=pltpu.VMEM)
    scratch = [
        vm(tokens.shape, BF16),
        vm(u_weight.shape, F32), vm(v_weight.shape, F32), vm(out_weight.shape, F32),
        vm(gate_weight.shape, F32), vm(up_weight.shape, F32), vm(down_weight.shape, F32),
        vm((2, 4, 4, depth, mix_cols), BF16), vm((2, 4, 4, depth, mix_cols), BF16),
        vm((2, 4, 4, mix_cols // 2, out_cols), BF16), vm((2, 4, 4, mix_cols // 2, out_cols), BF16),
        vm((2, 4, 4, depth, ff), BF16), vm((2, 4, 4, depth, ff), BF16),
        vm((2, 4, 4, ff // 2, out_cols), BF16), vm((2, 4, 4, ff // 2, out_cols), BF16),
        vm((4, rows, width), BF16), vm((4, rows, width), BF16),
        vm((4, rows, 2 * mix_cols), BF16), vm((4, rows, 2 * mix_cols), BF16), vm((4, rows, 2 * mix_cols), BF16),
        vm((2, 2 * rows, ff), BF16),
        vm((4, rows, width), BF16), vm((4, rows, width), BF16),
        vm((2, rows // 2, width), BF16), vm((2, rows // 2, width), BF16),
        vm((rows, width), BF16), vm((rows, width), BF16), vm((rows, width), BF16), vm((rows, width), BF16),
        vm((rows, width), BF16),
        vm((4, 8, BLK), F32), vm((3, 4, 8, BLK), F32), vm((2, 8, mix_cols), F32),
        pltpu.SemaphoreType.DMA((7,)),
        pltpu.SemaphoreType.DMA((N_SENDS,)),
        pltpu.SemaphoreType.DMA((8, N_GATHER_SEMS)),
        pltpu.SemaphoreType.DMA((24,)),
        pltpu.SemaphoreType.DMA((4,)),
    ]
    return pl.pallas_call(
        layer_kernel,
        out_shape=jax.ShapeDtypeStruct(tokens.shape, BF16),
        in_specs=[anywhere] * 7 + [on_chip] * 11,
        out_specs=on_chip,
        scratch_shapes=scratch,
        compiler_params=pltpu.CompilerParams(
            collective_id=0, has_side_effects=True, vmem_limit_bytes=60 * 1024 * 1024
        ),
    )(
        tokens, u_weight, v_weight, out_weight, gate_weight, up_weight, down_weight,
        row(mix_gain), row(ffn_gain), row(u_scale), row(v_scale), row(v_gain), row(out_scale),
        row(gate_scale), row(up_scale), row(down_scale), spatial_weight, bias,
    )


def solution(mesh):
    both = ("fs", "tp")
    in_specs = (
        P(both, None), P(), P(),
        P("fs", "tp"), P("tp"), P("fs", "tp"), P("tp"), P("tp"),
        P(), P(),
        P("tp", "fs"), P("fs"),
        P("fs", "tp"), P("tp"), P("fs", "tp"), P("tp"),
        P("tp", "fs"), P("fs"),
    )
    return jax.shard_map(local, mesh=mesh, in_specs=in_specs, out_specs=P(both, None), check_vma=False)
```

```python
import functools

import jax
import jax.numpy as jnp
from jax import lax
from jax.experimental import pallas as pl
from jax.experimental.pallas import tpu as pltpu
from jax.sharding import PartitionSpec as P

MESH = pl.DeviceIdType.MESH
F32 = jnp.float32
BF16 = jnp.bfloat16
A = 2048
BLK = 128
LEFT, RIGHT, OPP, OWN = 0, 1, 2, 3


def rms_rows(widened, norm_gain):
    factor = lax.rsqrt(jnp.mean(widened * widened, axis=1, keepdims=True) + 1e-06)
    return (widened * factor * norm_gain).astype(BF16)


def gelu(x):
    return 0.5 * x * (1.0 + jnp.tanh(0.7978845608028654 * (x + 0.044715 * (x * x * x))))


def silu(x):
    return 0.5 * x * (1.0 + jnp.tanh(0.5 * x))


ORDER = (
    184, 187, 185, 186, 235, 0, 1, 20, 21, 4, 5, 24,
    25, 2000, 136, 168, 1161, 44, 45, 64, 65, 40, 41, 60,
    61, 1000, 2, 6, 7, 1001, 3, 8, 9, 1012, 22, 26,
    27, 1013, 23, 28, 29, 1004, 12, 1016, 32, 1028, 1040, 1024,
    47, 1025, 43, 49, 1036, 67, 1037, 69, 1002, 42, 62, 63,
    52, 72, 1003, 16, 10, 11, 1110, 188, 1113, 189, 1006, 13,
    66, 1005, 1018, 33, 1017, 1008, 14, 1014, 68, 1015, 36, 30,
    31, 1020, 34, 1027, 1029, 46, 1041, 1032, 54, 48, 1026, 56,
    51, 1038, 1039, 76, 71, 1044, 74, 50, 70, 1009, 15, 18,
    1042, 73, 1111, 1112, 1007, 17, 1021, 35, 38, 1030, 53, 80,
    81, 100, 101, 1033, 58, 1045, 78, 1019, 37, 1010, 19, 1031,
    57, 1043, 77, 1022, 39, 55, 75, 104, 1114, 84, 85, 105,
    1115, 1011, 1023, 2001, 2002, 1048, 82, 1049, 1061, 2003, 83, 103,
    86, 1034, 59, 1046, 79, 1060, 2004, 233, 234, 232, 106, 1035,
    87, 107, 1047, 1064, 1159, 102, 1160, 1052, 1158, 2006, 2008, 204,
    205, 206, 207, 112, 2005, 2007, 202, 203, 92, 89, 109, 1050,
    1051, 96, 1063, 1054, 1066, 113, 1130, 93, 91, 1132, 2025, 208,
    1053, 1062, 116, 111, 1065, 2027, 210, 1131, 1133, 2026, 209, 2028,
    211, 108, 1056, 94, 88, 1068, 114, 110, 1128, 90, 1129, 1057,
    98, 95, 1069, 118, 115, 1134, 1136, 2037, 190, 191, 2039, 195,
    194, 120, 121, 152, 153, 1135, 1137, 2038, 192, 193, 2040, 197,
    196, 1067, 117, 124, 125, 156, 157, 1116, 198, 1117, 1055, 97,
    1058, 99, 1070, 119, 1072, 122, 140, 126, 127, 1073, 123, 144,
    1091, 172, 158, 1092, 176, 1120, 154, 155, 159, 1121, 200, 1095,
    169, 128, 129, 160, 1076, 137, 1077, 138, 1096, 170, 161, 1074,
    1118, 199, 1119, 1075, 148, 164, 1059, 130, 131, 1078, 141, 1079,
    142, 1097, 173, 1093, 1094, 180, 163, 1071, 1098, 174, 162, 133,
    1122, 1123, 201, 2009, 2010, 1099, 177, 1080, 145, 1081, 146, 134,
    2011, 132, 165, 1100, 178, 166, 2012, 1124, 1126, 2013, 1103, 171,
    1082, 149, 1083, 150, 135, 2014, 1102, 182, 167, 1088, 1107, 2021,
    212, 213, 1101, 181, 1085, 143, 1125, 1127, 2015, 1086, 147, 1090,
    2016, 1105, 179, 2017, 1104, 175, 1084, 139, 1109, 2018, 1087, 151,
    2019, 1106, 183, 2020, 2022, 214, 215, 216, 217, 1138, 1139, 1089,
    1108, 2024, 224, 225, 226, 227, 2023, 222, 223, 1140, 1142, 2029,
    218, 2031, 220, 1141, 1143, 2030, 219, 2032, 221, 1150, 1152, 2033,
    228, 2035, 230, 1151, 1153, 2034, 229, 2036, 231, 1148, 1149, 1144,
    1146, 1145, 1147, 2041, 1154, 1156, 1155, 1157, 2042,
)
N_FAMILIES, N_ARRIVALS = 31, 162


COLUMNS = (
    ((0, 0), (0, -1), (0, 1), (-1, 0), (1, 0), (-1, -1), (1, 1), (-1, 1)),
    ((1, -1), (2, 0), (0, 2), (2, 1), (1, 2), (2, -1), (-1, 2), (2, 2)),
)
OFFSETS = {"o": 0, "L": -1, "R": 1, "P": 2}


def weight_transfers(name, buf, x_first, place):
    x, y, z, c = place
    low, high = pl.ds(0, buf.shape[3] // 2), pl.ds(buf.shape[3] // 2, buf.shape[3] // 2)

    def at(value, step):
        return lax.rem(value + step + 4, 4)

    def block(a, b, rows=None):
        ref = buf.at[c, at(z, b), at(x, a)] if x_first else buf.at[c, at(z, a), at(x, b)]
        return ref if rows is None else ref.at[rows]

    def group(b, core=None):
        core = c if core is None else core
        return buf.at[core, at(z, b)] if x_first else buf.at[core, :, at(x, b)]

    def device(first, step):
        along_x = first == x_first
        return (z * 4 + at(x, step), y * 2 + c) if along_x else (at(z, step) * 4 + x, y * 2 + c)

    found = {}
    for sign, step in (("+", 1), ("-", -1)):
        rows = low if step == 1 else high
        found["1" + sign] = (block(0, 0), device(True, step), block(-step, 0))
        found["1f" + sign] = (block(-step, 0, rows), device(True, step), block(2, 0, rows))
        far = device(False, step)
        for kind, a in OFFSETS.items():
            found["2" + kind + sign] = (block(a, 0), far, block(a, -step))
            found["2f" + kind + sign] = (block(a, -step), far, block(a, 2))
    partner = (z * 4 + x, y * 2 + 1 - c)
    parts = {"d0": 0, "d-": -1, "d+": 1, "d2": 2}
    for kind, a in OFFSETS.items():
        for mark, b in (("o", 0), ("-", -1), ("+", 1), ("2", 2)):
            other = buf.at[1 - c, at(z, b), at(x, a)] if x_first else buf.at[1 - c, at(z, a), at(x, b)]
            found["e" + kind + mark] = (block(a, b), partner, other)
    for key, b in parts.items():
        found[key] = (group(b), partner, group(b, core=1 - c))
    shared = list(parts) if name[0] != "D" else ["e" + kind + mark for kind in OFFSETS for mark in "o-+2"]
    used = ["1+", "1-", "1f+", "1f-"] + ["2" + kind + sign for kind in OFFSETS for sign in "+-"]
    used += ["2fo+", "2fL+", "2fR-", "2fP-"] + shared
    return {name + ":" + key: (found[key][0],) + found[key] for key in used}


def arrival_group(name):
    head, _, key = name.partition(":")
    if key[0] == "e":
        early = key[1] != "P" and key[2] != "2"
        return (head, "ea", 9) if early else (head, "eb", 4) if key[2] == "2" else (head, "ec", 3)
    if head[0] != "D":
        if key[0] == "d":
            return head, "d", 16
        if key[:2] == "2f":
            return head, "2f", 4
        if key in ("2R+", "2P+"):
            return head, "2a", 2
        if key in ("2o-", "2L-"):
            return head, "2b", 2
    return head, key, 1


def layer_kernel(
    *refs,
):
    held_in_hbm, out_ref, held, refs = refs[:18], refs[18], refs[19:37], refs[37:]
    tok, mix_gain, u32, u_scale, v32, v_scale, o32, o_scale, v_gain, g32, g_scale, p32, p_scale, d32, d_scale, *rest = held
    spatial, bias, ffn_gain = rest
    (
        ub, vb, oab, obb, gb, pb, dab, dbb,
        x1, x2, u_val, v_val, gated, hid, part1, part2, relay1, relay2, fl1, fr1, fl2, fr2, res,
        stat, stat_in, vg,
        load_sems, send_sems, recv_sems,
    ) = refs
    fs = lax.axis_index("fs")
    tp = lax.axis_index("tp")
    z, x = fs // 4, lax.rem(fs, 4)
    y, c = tp // 2, lax.rem(tp, 2)
    partner = (fs, y * 2 + 1 - c)
    y_right = (fs, lax.rem(y + 1, 4) * 2 + c)
    y_left = (fs, lax.rem(y + 3, 4) * 2 + c)
    y_opp = (fs, lax.rem(y + 2, 4) * 2 + c)

    loads = []
    for n, (src, dst) in enumerate(zip(held_in_hbm, held)):
        copy = pltpu.make_async_copy(src, dst, load_sems.at[n])
        copy.start()
        loads.append((n, copy))

    barrier = pltpu.get_barrier_semaphore()
    plane = [
        (z * 4 + lax.rem(x + 1, 4), tp),
        (z * 4 + lax.rem(x + 3, 4), tp),
        (lax.rem(z + 1, 4) * 4 + x, tp),
        (lax.rem(z + 3, 4) * 4 + x, tp),
    ]
    peers = [partner, y_right, y_left, y_opp] + plane
    for peer in peers:
        pl.semaphore_signal(barrier, inc=1, device_id=peer, device_id_type=MESH)

    def ready(last):
        while loads[0][0] <= last:
            loads.pop(0)[1].wait()
            if not loads:
                break

    ready(3 + 2)
    ub[c, z, x] = (u32[...] * u_scale[...]).astype(BF16)
    vb[c, z, x] = (v32[...] * v_scale[...]).astype(BF16)
    x1[OWN] = rms_rows(tok[...].astype(F32), mix_gain[...])
    ready(8)
    half = o32.shape[0] // 2
    oab[c, z, x] = (o32[:half] * o_scale[...]).astype(BF16)
    obb[c, z, x] = (o32[half:] * o_scale[...]).astype(BF16)
    vg[c] = jnp.broadcast_to(v_gain[...], vg.shape[1:])

    pl.semaphore_wait(barrier, len(peers))


    moves = {}
    for n, (name, buf) in enumerate(
        (("U", ub), ("V", vb), ("OA", oab), ("OB", obb), ("G", gb), ("Q", pb), ("DA", dab), ("DB", dbb))
    ):
        moves.update(weight_transfers(name, buf, n % 2 == 0, (x, y, z, c)))

    H0, H1 = pl.ds(0, 64), pl.ds(64, 64)
    Q = [pl.ds(32 * q, 32) for q in range(4)]

    def rows_move(buf, to_right, rows):
        to = LEFT if to_right else RIGHT
        return (buf.at[OWN, rows], buf.at[to, rows], y_right if to_right else y_left, buf.at[to, rows])

    def pass_on(buf, to_right, rows):
        kept = LEFT if to_right else RIGHT
        return (buf.at[kept, rows], buf.at[OPP, rows], y_right if to_right else y_left, buf.at[OPP, rows])

    moves["X1:H0+"] = rows_move(x1, True, H0)
    moves["X1:H0-"] = rows_move(x1, False, H0)
    moves["X1:H1+"] = rows_move(x1, True, H1)
    moves["X1:H1-"] = rows_move(x1, False, H1)
    moves["X1:f+"] = pass_on(x1, True, H0)
    moves["X1:f-"] = pass_on(x1, False, H1)
    for q in range(4):
        moves[f"X2:{q}+"] = rows_move(x2, True, Q[q])
        moves[f"X2:{q}-"] = rows_move(x2, False, Q[q])
    for q in range(4):
        moves[f"X2:f{q}"] = pass_on(x2, q < 2, Q[q])
    for key, part, relay, fl, fr in (
        ("S1", part1, relay1, fl1, fr1),
        ("S2", part2.at[0], relay2.at[0], fl2.at[0], fr2.at[0]),
        ("S3", part2.at[1], relay2.at[1], fl2.at[1], fr2.at[1]),
    ):
        moves[f"{key}:n+"] = (part.at[RIGHT, H1], fl.at[H1], y_right, fl.at[H1])
        moves[f"{key}:n-"] = (part.at[LEFT, H0], fr.at[H0], y_left, fr.at[H0])
        for q in range(4):
            to = y_right if q < 2 else y_left
            moves[f"{key}:o{q}"] = (part.at[OPP, Q[q]], relay.at[Q[q]], to, relay.at[Q[q]])
        for q in range(4):
            near, into, to = (RIGHT, fl, y_right) if q < 2 else (LEFT, fr, y_left)
            moves[f"{key}:r{q}"] = (part.at[near, Q[q]], into.at[Q[q]], to, into.at[Q[q]])
    moves["stat:R"] = (stat, stat_in.at[0], y_right, stat_in.at[0])
    moves["stat:L"] = (stat, stat_in.at[1], y_left, stat_in.at[1])
    moves["stat:P"] = (stat, stat_in.at[2], y_opp, stat_in.at[2])
    moves["vg"] = (vg.at[c], vg.at[c], partner, vg.at[1 - c])

    slot_chip = [lax.rem(y + 3, 4), lax.rem(y + 1, 4), lax.rem(y + 2, 4), y]
    row_ids = lax.broadcasted_iota(jnp.int32, (BLK, BLK), 0)
    col_ids = lax.broadcasted_iota(jnp.int32, (BLK, BLK), 1)
    eye = row_ids == col_ids

    def project_mixer(first, core):
        rows = x1[first : first + 2].reshape(2 * BLK, -1)
        cols = slice(core * 256, core * 256 + 256)
        u = gelu(jnp.dot(rows, ub[core].reshape(A, 256), preferred_element_type=F32))
        v = gelu(jnp.dot(rows, vb[core].reshape(A, 256), preferred_element_type=F32)).astype(BF16)
        u_val[first : first + 2, :, cols] = u.astype(BF16).reshape(2, BLK, 256)
        v_val[first : first + 2, :, cols] = v.reshape(2, BLK, 256)
        wide = v.astype(F32)
        columns = jnp.sum(wide, axis=1, keepdims=True), jnp.sum(wide * wide, axis=1, keepdims=True)
        for k in range(2):
            chip = slot_chip[first + k]
            for row in range(2):
                piece = columns[row][k * BLK : (k + 1) * BLK]
                turned = jnp.sum(jnp.where(eye, piece, 0.0), axis=0, keepdims=True)
                if core == 1:
                    turned = turned + stat[chip, row : row + 1, :]
                stat[chip, row : row + 1, :] = turned

    def mixing_rows(core):
        masked = jnp.where(col_ids <= row_ids, spatial[2 * y + core].astype(F32), 0.0)
        offset = jnp.sum(jnp.where(eye, bias[2 * y + core], 0.0), axis=1, keepdims=True)
        return masked, offset

    def mix(slot):
        chip = slot_chip[slot]
        total = stat[chip] + stat_in[0, chip] + stat_in[1, chip] + stat_in[2, chip]
        average = total[0:1] * (1.0 / A)
        spread = total[1:2] * (1.0 / A) - average * average
        factor = lax.rsqrt(spread + 1e-05)
        for core in range(2):
            cols = slice(core * 256, core * 256 + 256)
            masked, offset = mixing_rows(core)
            scaled = (masked * factor).astype(BF16)
            shift = jnp.sum(scaled.astype(F32) * average, axis=1, keepdims=True)
            mixed = jnp.dot(scaled, v_val[slot, :, cols], preferred_element_type=F32)
            mixed = (mixed - shift) * vg[core, 0:1, :] + offset
            gated[slot, :, cols] = (u_val[slot, :, cols].astype(F32) * mixed).astype(BF16)

    def project_out(first):
        rows = gated[first : first + 2].reshape(2 * BLK, -1)
        for j in range(8):
            fz, fx = j // 2, (j % 2) * 2
            matrix = jnp.concatenate(
                [
                    jnp.concatenate([buf[core, fz, fx + k] for core in range(2) for buf in (oab, obb)], axis=0)
                    for k in range(2)
                ],
                axis=1,
            )
            total = jnp.dot(rows, matrix, preferred_element_type=F32)
            part1[first : first + 2, :, j * 256 : j * 256 + 256] = total.astype(BF16).reshape(2, BLK, 256)

    def project_ffn(first, n):
        rows = x2[first : first + 2].reshape(2 * BLK, -1)
        core, j = n // 3, n % 3
        cols = slice(j * 256, j * 256 + 256)
        gate = jnp.dot(rows, gb[core, :, :, :, cols].reshape(A, 256), preferred_element_type=F32)
        up = jnp.dot(rows, pb[core, :, :, :, cols].reshape(A, 256), preferred_element_type=F32)
        hid[first // 2, :, n * 256 : n * 256 + 256] = (silu(gate) * up).astype(BF16)

    def place_of(dz, dx):
        return lax.rem(z + dz + 4, 4), lax.rem(x + dx + 4, 4)

    def project_down(first, part):
        rows = hid[first // 2]
        for j in range(0, 8, 2):
            pair = []
            for dz, dx in COLUMNS[part][j : j + 2]:
                fz, fx = place_of(dz, dx)
                pair.append(
                    jnp.concatenate([buf[core, fz, fx] for core in range(2) for buf in (dab, dbb)], axis=0)
                )
            total = jnp.dot(rows, jnp.concatenate(pair, axis=1), preferred_element_type=F32)
            cols = slice(j * BLK, j * BLK + 256)
            part2[part, first : first + 2, :, cols] = total.astype(BF16).reshape(2, BLK, 256)

    def add_relayed(part, relay, q):
        near = RIGHT if q < 2 else LEFT
        part[near, Q[q]] = (part[near, Q[q]].astype(F32) + relay[Q[q]].astype(F32)).astype(BF16)

    def second_norm(q):
        total = tok[Q[q]].astype(F32) + part1[OWN, Q[q]].astype(F32)
        residual = (total + fl1[Q[q]].astype(F32) + fr1[Q[q]].astype(F32)).astype(BF16)
        res[Q[q]] = residual
        x2[OWN, Q[q]] = rms_rows(residual.astype(F32), ffn_gain[...])

    def finish(part):
        for j, (dz, dx) in enumerate(COLUMNS[part]):
            fz, fx = place_of(dz, dx)
            cols = pl.ds(pl.multiple_of((fz * 4 + fx) * BLK, BLK), BLK)
            held = slice(j * BLK, j * BLK + BLK)
            total = res[:, cols].astype(F32) + part2[part, OWN, :, held].astype(F32)
            total = total + fl2[part, :, held].astype(F32) + fr2[part, :, held].astype(F32)
            out_ref[:, cols] = total

    def convert_rest():
        ready(14)
        gb[c, z, x] = (g32[...] * g_scale[...].reshape(1, -1)).astype(BF16)
        pb[c, z, x] = (p32[...] * p_scale[...].reshape(1, -1)).astype(BF16)
        half = d32.shape[0] // 2
        dab[c, z, x] = (d32[:half] * d_scale[...]).astype(BF16)
        dbb[c, z, x] = (d32[half:] * d_scale[...]).astype(BF16)
        stat[...] = jnp.zeros_like(stat)
        ready(17)

    halves = (LEFT, OPP)
    work = [convert_rest]
    work += [functools.partial(project_mixer, first, core) for first in halves for core in range(2)]
    work += [lambda: (mix(LEFT), mix(RIGHT)), lambda: (mix(OPP), mix(OWN))]
    work += [functools.partial(project_out, first) for first in halves]
    work += [functools.partial(project_ffn, first, n) for first in halves for n in range(6)]
    work += [functools.partial(project_down, first, part) for part in range(2) for first in halves]
    for part, relay in ((part1, relay1), (part2.at[0], relay2.at[0]), (part2.at[1], relay2.at[1])):
        work += [functools.partial(add_relayed, part, relay, q) for q in range(4)]
    work += [functools.partial(second_norm, q) for q in range(4)]
    work += [functools.partial(finish, part) for part in range(2)]

    families = {}
    for n, buf in (("U", ub), ("V", vb), ("OA", oab), ("OB", obb), ("G", gb), ("Q", pb), ("DA", dab), ("DB", dbb)):
        families[n + "1"] = buf.at[0, 0, pl.ds(0, 3)]
        families[n + "2"] = buf.at[0, pl.ds(0, 3)]
        families[n + "s"] = buf.at[0]
    families["X1"], families["X2"], families["S1"] = x1.at[pl.ds(0, 3)], x2.at[pl.ds(0, 3)], part1.at[pl.ds(0, 3)]
    families["S2"], families["S3"] = part2.at[0, pl.ds(0, 3)], part2.at[1, pl.ds(0, 3)]
    families["stat"], families["vg"] = stat_in, vg.at[0]
    family_sem = {name: n for n, name in enumerate(families)}

    def family_of(name):
        head, _, tail = name.partition(":")
        if head in families:
            return head
        return head + (tail[0] if tail[0] in "12" else "s")

    buffers = {"U": ub, "V": vb, "OA": oab, "OB": obb, "G": gb, "Q": pb, "DA": dab, "DB": dbb}
    arrivals, arrival_of = [], {}
    known = {}
    for name, (_, _, to, ref) in moves.items():
        head = name.partition(":")[0]
        key = name
        if head in buffers:
            key = arrival_group(name)
            buf, blocks = buffers[head], key[2]
            if blocks > 1:
                ref = {16: buf.at[0], 9: buf.at[0, pl.ds(0, 3), pl.ds(0, 3)]}.get(blocks)
                ref = buf.at[0, 0, pl.ds(0, blocks)] if ref is None else ref
        if key not in known:
            known[key] = len(arrivals)
            arrivals.append((ref, to))
        arrival_of[name] = known[key]
    names = list(moves)

    def start(n):
        name = names[n]
        src, dst, to, _ = moves[name]
        pltpu.make_async_remote_copy(
            src_ref=src, dst_ref=dst, send_sem=send_sems.at[family_sem[family_of(name)]],
            recv_sem=recv_sems.at[arrival_of[name]], device_id=to, device_id_type=MESH,
        ).start()

    def arrive(n):
        ref, to = arrivals[n]
        sem = recv_sems.at[n]
        pltpu.make_async_remote_copy(
            src_ref=ref, dst_ref=ref, send_sem=sem, recv_sem=sem, device_id=to, device_id_type=MESH
        ).wait_recv()

    acts = (start, arrive, lambda n: work[n]())
    for code in ORDER:
        step = functools.partial(acts[code // 1000], code % 1000)
        step()
    for name, ref in families.items():
        sem = send_sems.at[family_sem[name]]
        pltpu.make_async_remote_copy(
            src_ref=ref, dst_ref=ref, send_sem=sem, recv_sem=sem, device_id=partner, device_id_type=MESH
        ).wait_send()


def local(
    tokens, mix_gain, ffn_gain, u_weight, u_scale, v_weight, v_scale, v_gain, spatial_weight, spatial_bias,
    out_weight, out_scale, gate_weight, gate_scale, up_weight, up_scale, down_weight, down_scale,
):
    rows, width = tokens.shape
    row = lambda a: a.reshape(1, -1)
    bias = spatial_bias.reshape(spatial_bias.shape[0], 1, BLK)
    depth = u_weight.shape[0]
    ff = gate_weight.shape[1]
    mix_cols = u_weight.shape[1]
    out_cols = out_weight.shape[1]
    vm = pltpu.VMEM
    on_chip = pl.BlockSpec(memory_space=pltpu.VMEM)
    inputs = (
        tokens, row(mix_gain), u_weight, row(u_scale), v_weight, row(v_scale), out_weight, row(out_scale), row(v_gain),
        gate_weight, gate_scale, up_weight, up_scale, down_weight, row(down_scale), spatial_weight, bias, row(ffn_gain),
    )
    in_hbm = pl.BlockSpec(memory_space=pltpu.HBM)
    scratch = [vm(a.shape, a.dtype) for a in inputs] + [
        vm((2, 4, 4, depth, mix_cols), BF16), vm((2, 4, 4, depth, mix_cols), BF16),
        vm((2, 4, 4, mix_cols // 2, out_cols), BF16), vm((2, 4, 4, mix_cols // 2, out_cols), BF16),
        vm((2, 4, 4, depth, ff), BF16), vm((2, 4, 4, depth, ff), BF16),
        vm((2, 4, 4, ff // 2, out_cols), BF16), vm((2, 4, 4, ff // 2, out_cols), BF16),
        vm((4, rows, width), BF16), vm((4, rows, width), BF16),
        vm((4, rows, 2 * mix_cols), BF16), vm((4, rows, 2 * mix_cols), BF16), vm((4, rows, 2 * mix_cols), BF16),
        vm((2, 2 * rows, 2 * ff), BF16),
        vm((4, rows, width), BF16), vm((2, 4, rows, width // 2), BF16),
        vm((rows, width), BF16), vm((2, rows, width // 2), BF16),
        vm((rows, width), BF16), vm((rows, width), BF16),
        vm((2, rows, width // 2), BF16), vm((2, rows, width // 2), BF16),
        vm((rows, width), BF16),
        vm((4, 8, BLK), F32), vm((3, 4, 8, BLK), F32), vm((2, 8, mix_cols), F32),
        pltpu.SemaphoreType.DMA((len(inputs),)),
        pltpu.SemaphoreType.DMA((N_FAMILIES,)),
        pltpu.SemaphoreType.DMA((N_ARRIVALS,)),
    ]
    summed = pl.pallas_call(
        layer_kernel,
        out_shape=jax.ShapeDtypeStruct(tokens.shape, F32),
        in_specs=[in_hbm] * len(inputs),
        out_specs=on_chip,
        scratch_shapes=scratch,
        compiler_params=pltpu.CompilerParams(
            collective_id=0, has_side_effects=True, vmem_limit_bytes=60 * 1024 * 1024
        ),
    )(*inputs)
    return summed.astype(BF16)


def solution(mesh):
    both = ("fs", "tp")
    in_specs = (
        P(both, None), P(), P(),
        P("fs", "tp"), P("tp"), P("fs", "tp"), P("tp"), P("tp"),
        P(), P(),
        P("tp", "fs"), P("fs"),
        P("fs", "tp"), P("tp"), P("fs", "tp"), P("tp"),
        P("tp", "fs"), P("fs"),
    )
    return jax.shard_map(local, mesh=mesh, in_specs=in_specs, out_specs=P(both, None), check_vma=False)
```

```python
import functools

import jax
import jax.numpy as jnp
from jax import lax
from jax.experimental import pallas as pl
from jax.experimental.pallas import tpu as pltpu
from jax.sharding import PartitionSpec as P

MESH = pl.DeviceIdType.MESH
F32 = jnp.float32
BF16 = jnp.bfloat16
A = 2048
BLK = 128
LEFT, RIGHT, OPP, OWN = 0, 1, 2, 3


def rms_rows(widened, norm_gain):
    factor = lax.rsqrt(jnp.mean(widened * widened, axis=1, keepdims=True) + 1e-06)
    return (widened * factor * norm_gain).astype(BF16)


def gelu(x):
    return 0.5 * x * (1.0 + jnp.tanh(0.7978845608028654 * (x + 0.044715 * (x * x * x))))


def silu(x):
    return 0.5 * x * (1.0 + jnp.tanh(0.5 * x))


ORDER = (
    184, 187, 185, 186, 235, 0, 1, 20, 21, 4, 5, 24,
    25, 2000, 136, 168, 1133, 44, 45, 64, 65, 40, 41, 60,
    61, 1000, 2, 6, 7, 1001, 3, 8, 9, 1011, 22, 26,
    27, 1012, 23, 28, 29, 1003, 12, 1014, 32, 1025, 1036, 1022,
    47, 1023, 43, 49, 1033, 67, 1034, 1102, 188, 42, 62, 63,
    52, 72, 69, 1104, 189, 1002, 16, 10, 11, 1005, 13, 1004,
    1016, 33, 1015, 1007, 14, 66, 1013, 36, 30, 31, 1018, 34,
    1026, 1037, 46, 1029, 54, 1040, 74, 48, 68, 1024, 56, 51,
    1035, 76, 71, 50, 70, 1103, 1008, 18, 15, 1006, 17, 1019,
    38, 35, 1038, 73, 1027, 53, 1030, 58, 55, 1017, 37, 1041,
    78, 75, 1028, 57, 1039, 77, 80, 81, 100, 101, 1009, 19,
    1105, 1020, 39, 84, 85, 104, 105, 1010, 1021, 2001, 2002, 233,
    234, 232, 1031, 59, 1042, 79, 1032, 1043, 1044, 82, 86, 87,
    1055, 107, 1056, 1045, 106, 1132, 2004, 2006, 204, 205, 206, 207,
    83, 102, 103, 2003, 2005, 202, 203, 1047, 1058, 92, 112, 89,
    109, 1049, 1048, 1059, 1114, 1116, 2017, 208, 2019, 210, 93, 108,
    1057, 116, 111, 1060, 1046, 96, 91, 1115, 1117, 2018, 209, 2020,
    211, 1051, 94, 113, 88, 1062, 114, 1112, 1113, 1052, 98, 95,
    90, 110, 1063, 118, 115, 1118, 1120, 2029, 190, 191, 2031, 195,
    194, 1119, 1121, 2030, 192, 193, 2032, 197, 196, 120, 121, 152,
    153, 1106, 198, 124, 125, 156, 157, 1050, 97, 1053, 99, 1061,
    117, 1064, 119, 1109, 200, 1066, 122, 140, 126, 127, 1084, 172,
    159, 1085, 176, 1067, 144, 158, 123, 154, 155, 1108, 199, 128,
    129, 160, 161, 1069, 137, 1070, 138, 1087, 169, 1088, 170, 1054,
    1107, 132, 164, 1110, 201, 1071, 141, 1072, 142, 1090, 174, 1068,
    148, 131, 1086, 180, 163, 1089, 173, 1065, 2007, 133, 165, 2008,
    2009, 130, 162, 1073, 145, 1074, 146, 134, 1091, 177, 1092, 178,
    166, 1111, 2010, 1077, 139, 1095, 171, 2011, 1076, 150, 135, 1094,
    182, 167, 2012, 1078, 143, 1096, 175, 1081, 1099, 2014, 214, 215,
    216, 217, 2013, 212, 213, 1075, 149, 1079, 147, 1093, 181, 1097,
    179, 1080, 151, 1098, 183, 1123, 1125, 2021, 218, 2023, 220, 1083,
    1101, 1124, 1126, 2022, 219, 2024, 221, 1082, 1100, 2016, 224, 225,
    226, 227, 2015, 222, 223, 1122, 2033, 1128, 1130, 2025, 228, 2027,
    230, 1129, 1131, 2026, 229, 2028, 231, 1127, 2034,
)
N_FAMILIES, N_ARRIVALS = 19, 134


COLUMNS = (
    ((0, 0), (0, -1), (0, 1), (-1, 0), (1, 0), (-1, -1), (1, 1), (-1, 1)),
    ((1, -1), (2, 0), (0, 2), (2, 1), (1, 2), (2, -1), (-1, 2), (2, 2)),
)
OFFSETS = {"o": 0, "L": -1, "R": 1, "P": 2}


def weight_transfers(name, buf, x_first, place):
    x, y, z, c = place
    low, high = pl.ds(0, buf.shape[3] // 2), pl.ds(buf.shape[3] // 2, buf.shape[3] // 2)

    def at(value, step):
        return lax.rem(value + step + 4, 4)

    def block(a, b, rows=None):
        ref = buf.at[c, at(z, b), at(x, a)] if x_first else buf.at[c, at(z, a), at(x, b)]
        return ref if rows is None else ref.at[rows]

    def group(b, core=None):
        core = c if core is None else core
        return buf.at[core, at(z, b)] if x_first else buf.at[core, :, at(x, b)]

    def device(first, step):
        along_x = first == x_first
        return (z * 4 + at(x, step), y * 2 + c) if along_x else (at(z, step) * 4 + x, y * 2 + c)

    found = {}
    for sign, step in (("+", 1), ("-", -1)):
        rows = low if step == 1 else high
        found["1" + sign] = (block(0, 0), device(True, step), block(-step, 0))
        found["1f" + sign] = (block(-step, 0, rows), device(True, step), block(2, 0, rows))
        far = device(False, step)
        for kind, a in OFFSETS.items():
            found["2" + kind + sign] = (block(a, 0), far, block(a, -step))
            found["2f" + kind + sign] = (block(a, -step), far, block(a, 2))
    partner = (z * 4 + x, y * 2 + 1 - c)
    parts = {"d0": 0, "d-": -1, "d+": 1, "d2": 2}
    for kind, a in OFFSETS.items():
        for mark, b in (("o", 0), ("-", -1), ("+", 1), ("2", 2)):
            other = buf.at[1 - c, at(z, b), at(x, a)] if x_first else buf.at[1 - c, at(z, a), at(x, b)]
            found["e" + kind + mark] = (block(a, b), partner, other)
    for key, b in parts.items():
        found[key] = (group(b), partner, group(b, core=1 - c))
    shared = list(parts) if name[0] != "D" else ["e" + kind + mark for kind in OFFSETS for mark in "o-+2"]
    used = ["1+", "1-", "1f+", "1f-"] + ["2" + kind + sign for kind in OFFSETS for sign in "+-"]
    used += ["2fo+", "2fL+", "2fR-", "2fP-"] + shared
    return {name + ":" + key: (found[key][0],) + found[key] for key in used}


def arrival_group(name):
    head, _, key = name.partition(":")
    if key[:2] == "1f":
        return head, "1f", 1
    if key[0] == "e":
        early = key[1] != "P" and key[2] != "2"
        return (head, "ea", 9) if early else (head, "eb", 4) if key[2] == "2" else (head, "ec", 3)
    if head[0] != "D":
        if key[0] == "d":
            return head, "d", 16
        if key[:2] == "2f":
            return head, "2f", 4
        if key in ("2R+", "2P+"):
            return head, "2a", 2
        if key in ("2o-", "2L-"):
            return head, "2b", 2
    return head, key, 0


def layer_kernel(
    *refs,
):
    held_in_hbm, out_ref, held, refs = refs[:18], refs[18], refs[19:37], refs[37:]
    tok, mix_gain, u32, u_scale, v32, v_scale, o32, o_scale, v_gain, g32, g_scale, p32, p_scale, d32, d_scale, *rest = held
    spatial, bias, ffn_gain = rest
    (
        ub, vb, oab, obb, gb, pb, dab, dbb,
        x1, x2, u_val, v_val, gated, hid, part1, part2, relay1, relay2, fl1, fr1, fl2, fr2, res,
        stat, stat_in, vg,
        load_sems, send_sems, recv_sems,
    ) = refs
    fs = lax.axis_index("fs")
    tp = lax.axis_index("tp")
    z, x = fs // 4, lax.rem(fs, 4)
    y, c = tp // 2, lax.rem(tp, 2)
    partner = (fs, y * 2 + 1 - c)
    y_right = (fs, lax.rem(y + 1, 4) * 2 + c)
    y_left = (fs, lax.rem(y + 3, 4) * 2 + c)
    y_opp = (fs, lax.rem(y + 2, 4) * 2 + c)

    loads = []
    for n, (src, dst) in enumerate(zip(held_in_hbm, held)):
        copy = pltpu.make_async_copy(src, dst, load_sems.at[n])
        copy.start()
        loads.append((n, copy))

    barrier = pltpu.get_barrier_semaphore()
    plane = [
        (z * 4 + lax.rem(x + 1, 4), tp),
        (z * 4 + lax.rem(x + 3, 4), tp),
        (lax.rem(z + 1, 4) * 4 + x, tp),
        (lax.rem(z + 3, 4) * 4 + x, tp),
    ]
    peers = [partner, y_right, y_left, y_opp] + plane
    for peer in peers:
        pl.semaphore_signal(barrier, inc=1, device_id=peer, device_id_type=MESH)

    def ready(last):
        while loads[0][0] <= last:
            loads.pop(0)[1].wait()
            if not loads:
                break

    ready(3 + 2)
    ub[c, z, x] = (u32[...] * u_scale[...]).astype(BF16)
    vb[c, z, x] = (v32[...] * v_scale[...]).astype(BF16)
    x1[OWN] = rms_rows(tok[...].astype(F32), mix_gain[...])
    ready(8)
    half = o32.shape[0] // 2
    oab[c, z, x] = (o32[:half] * o_scale[...]).astype(BF16)
    obb[c, z, x] = (o32[half:] * o_scale[...]).astype(BF16)
    vg[c] = jnp.broadcast_to(v_gain[...], vg.shape[1:])

    pl.semaphore_wait(barrier, len(peers))


    moves = {}
    for n, (name, buf) in enumerate(
        (("U", ub), ("V", vb), ("OA", oab), ("OB", obb), ("G", gb), ("Q", pb), ("DA", dab), ("DB", dbb))
    ):
        moves.update(weight_transfers(name, buf, n % 2 == 0, (x, y, z, c)))

    H0, H1 = pl.ds(0, 64), pl.ds(64, 64)
    Q = [pl.ds(32 * q, 32) for q in range(4)]

    def rows_move(buf, to_right, rows):
        to = LEFT if to_right else RIGHT
        return (buf.at[OWN, rows], buf.at[to, rows], y_right if to_right else y_left, buf.at[to, rows])

    def pass_on(buf, to_right, rows):
        kept = LEFT if to_right else RIGHT
        return (buf.at[kept, rows], buf.at[OPP, rows], y_right if to_right else y_left, buf.at[OPP, rows])

    moves["X1:H0+"] = rows_move(x1, True, H0)
    moves["X1:H0-"] = rows_move(x1, False, H0)
    moves["X1:H1+"] = rows_move(x1, True, H1)
    moves["X1:H1-"] = rows_move(x1, False, H1)
    moves["X1:f+"] = pass_on(x1, True, H0)
    moves["X1:f-"] = pass_on(x1, False, H1)
    for q in range(4):
        moves[f"X2:{q}+"] = rows_move(x2, True, Q[q])
        moves[f"X2:{q}-"] = rows_move(x2, False, Q[q])
    for q in range(4):
        moves[f"X2:f{q}"] = pass_on(x2, q < 2, Q[q])
    for key, part, relay, fl, fr in (
        ("S1", part1, relay1, fl1, fr1),
        ("S2", part2.at[0], relay2.at[0], fl2.at[0], fr2.at[0]),
        ("S3", part2.at[1], relay2.at[1], fl2.at[1], fr2.at[1]),
    ):
        moves[f"{key}:n+"] = (part.at[RIGHT, H1], fl.at[H1], y_right, fl.at[H1])
        moves[f"{key}:n-"] = (part.at[LEFT, H0], fr.at[H0], y_left, fr.at[H0])
        for q in range(4):
            to = y_right if q < 2 else y_left
            moves[f"{key}:o{q}"] = (part.at[OPP, Q[q]], relay.at[Q[q]], to, relay.at[Q[q]])
        for q in range(4):
            near, into, to = (RIGHT, fl, y_right) if q < 2 else (LEFT, fr, y_left)
            moves[f"{key}:r{q}"] = (part.at[near, Q[q]], into.at[Q[q]], to, into.at[Q[q]])
    moves["stat:R"] = (stat, stat_in.at[0], y_right, stat_in.at[0])
    moves["stat:L"] = (stat, stat_in.at[1], y_left, stat_in.at[1])
    moves["stat:P"] = (stat, stat_in.at[2], y_opp, stat_in.at[2])
    moves["vg"] = (vg.at[c], vg.at[c], partner, vg.at[1 - c])

    slot_chip = [lax.rem(y + 3, 4), lax.rem(y + 1, 4), lax.rem(y + 2, 4), y]
    row_ids = lax.broadcasted_iota(jnp.int32, (BLK, BLK), 0)
    col_ids = lax.broadcasted_iota(jnp.int32, (BLK, BLK), 1)
    eye = row_ids == col_ids

    def project_mixer(first):
        rows = x1[first : first + 2].reshape(2 * BLK, -1)
        sums = squares = 0.0
        for core in range(2):
            cols = slice(core * 256, core * 256 + 256)
            u = gelu(jnp.dot(rows, ub[core].reshape(A, 256), preferred_element_type=F32))
            v = gelu(jnp.dot(rows, vb[core].reshape(A, 256), preferred_element_type=F32)).astype(BF16)
            u_val[first : first + 2, :, cols] = u.astype(BF16).reshape(2, BLK, 256)
            v_val[first : first + 2, :, cols] = v.reshape(2, BLK, 256)
            wide = v.astype(F32)
            sums = sums + jnp.sum(wide, axis=1, keepdims=True)
            squares = squares + jnp.sum(wide * wide, axis=1, keepdims=True)
        for k in range(2):
            for row, column in ((0, sums), (1, squares)):
                piece = column[k * BLK : (k + 1) * BLK]
                stat[slot_chip[first + k], row : row + 1, :] = jnp.sum(
                    jnp.where(eye, piece, 0.0), axis=0, keepdims=True
                )

    def mixing_rows(core):
        masked = jnp.where(col_ids <= row_ids, spatial[2 * y + core].astype(F32), 0.0)
        offset = jnp.sum(jnp.where(eye, bias[2 * y + core], 0.0), axis=1, keepdims=True)
        return masked, offset

    def mix(slot):
        chip = slot_chip[slot]
        total = stat[chip] + stat_in[0, chip] + stat_in[1, chip] + stat_in[2, chip]
        average = total[0:1] * (1.0 / A)
        spread = total[1:2] * (1.0 / A) - average * average
        factor = lax.rsqrt(spread + 1e-05)
        for core in range(2):
            cols = slice(core * 256, core * 256 + 256)
            masked, offset = mixing_rows(core)
            scaled = (masked * factor).astype(BF16)
            shift = jnp.sum(scaled.astype(F32) * average, axis=1, keepdims=True)
            mixed = jnp.dot(scaled, v_val[slot, :, cols], preferred_element_type=F32)
            mixed = (mixed - shift) * vg[core, 0:1, :] + offset
            gated[slot, :, cols] = (u_val[slot, :, cols].astype(F32) * mixed).astype(BF16)

    def project_out(first):
        rows = gated[first : first + 2].reshape(2 * BLK, -1)
        for j in range(8):
            fz, fx = j // 2, (j % 2) * 2
            matrix = jnp.concatenate(
                [
                    jnp.concatenate([buf[core, fz, fx + k] for core in range(2) for buf in (oab, obb)], axis=0)
                    for k in range(2)
                ],
                axis=1,
            )
            total = jnp.dot(rows, matrix, preferred_element_type=F32)
            part1[first : first + 2, :, j * 256 : j * 256 + 256] = total.astype(BF16).reshape(2, BLK, 256)

    def project_ffn(first, part):
        rows = x2[first : first + 2].reshape(2 * BLK, -1)
        for n in (2 * part, 2 * part + 1):
            core, j = n // 3, n % 3
            cols = slice(j * 256, j * 256 + 256)
            gate = jnp.dot(rows, gb[core, :, :, :, cols].reshape(A, 256), preferred_element_type=F32)
            up = jnp.dot(rows, pb[core, :, :, :, cols].reshape(A, 256), preferred_element_type=F32)
            hid[first // 2, :, n * 256 : n * 256 + 256] = (silu(gate) * up).astype(BF16)

    def place_of(dz, dx):
        return lax.rem(z + dz + 4, 4), lax.rem(x + dx + 4, 4)

    def project_down(first, part):
        rows = hid[first // 2]
        for j in range(0, 8, 2):
            pair = []
            for dz, dx in COLUMNS[part][j : j + 2]:
                fz, fx = place_of(dz, dx)
                pair.append(
                    jnp.concatenate([buf[core, fz, fx] for core in range(2) for buf in (dab, dbb)], axis=0)
                )
            total = jnp.dot(rows, jnp.concatenate(pair, axis=1), preferred_element_type=F32)
            cols = slice(j * BLK, j * BLK + 256)
            part2[part, first : first + 2, :, cols] = total.astype(BF16).reshape(2, BLK, 256)

    def add_relayed(part, relay, q):
        near = RIGHT if q < 2 else LEFT
        part[near, Q[q]] = (part[near, Q[q]].astype(F32) + relay[Q[q]].astype(F32)).astype(BF16)

    def second_norm(q):
        total = tok[Q[q]].astype(F32) + part1[OWN, Q[q]].astype(F32)
        residual = (total + fl1[Q[q]].astype(F32) + fr1[Q[q]].astype(F32)).astype(BF16)
        res[Q[q]] = residual
        x2[OWN, Q[q]] = rms_rows(residual.astype(F32), ffn_gain[...])

    def finish(part):
        for j, (dz, dx) in enumerate(COLUMNS[part]):
            fz, fx = place_of(dz, dx)
            cols = pl.ds(pl.multiple_of((fz * 4 + fx) * BLK, BLK), BLK)
            held = slice(j * BLK, j * BLK + BLK)
            total = res[:, cols].astype(F32) + part2[part, OWN, :, held].astype(F32)
            total = total + fl2[part, :, held].astype(F32) + fr2[part, :, held].astype(F32)
            out_ref[:, cols] = total.astype(BF16)

    def convert_rest():
        ready(14)
        gb[c, z, x] = (g32[...] * g_scale[...].reshape(1, -1)).astype(BF16)
        pb[c, z, x] = (p32[...] * p_scale[...].reshape(1, -1)).astype(BF16)
        half = d32.shape[0] // 2
        dab[c, z, x] = (d32[:half] * d_scale[...]).astype(BF16)
        dbb[c, z, x] = (d32[half:] * d_scale[...]).astype(BF16)
        stat[...] = jnp.zeros_like(stat)
        ready(17)

    halves = (LEFT, OPP)
    work = [convert_rest]
    work += [functools.partial(project_mixer, first) for first in halves]
    work += [lambda: (mix(LEFT), mix(RIGHT)), lambda: (mix(OPP), mix(OWN))]
    work += [functools.partial(project_out, first) for first in halves]
    work += [functools.partial(project_ffn, first, n) for first in halves for n in range(3)]
    work += [functools.partial(project_down, first, part) for part in range(2) for first in halves]
    for part, relay in ((part1, relay1), (part2.at[0], relay2.at[0]), (part2.at[1], relay2.at[1])):
        work += [functools.partial(add_relayed, part, relay, q) for q in range(4)]
    work += [functools.partial(second_norm, q) for q in range(4)]
    work += [functools.partial(finish, part) for part in range(2)]

    families = {}
    for n, buf in (("U", ub), ("O", oab), ("G", gb), ("D", dab)):
        families[n + "1"] = buf.at[:, 0, pl.ds(0, 3)]
        families[n + "2"] = buf.at[:, pl.ds(0, 3)]
        families[n + "s"] = buf
    families["X1"], families["X2"], families["S1"] = x1.at[pl.ds(0, 3)], x2.at[pl.ds(0, 3)], part1.at[pl.ds(0, 3)]
    families["S2"], families["S3"] = part2.at[0, pl.ds(0, 3)], part2.at[1, pl.ds(0, 3)]
    families["stat"], families["vg"] = stat_in, vg.at[0]
    family_sem = {name: n for n, name in enumerate(families)}

    def family_of(name):
        head, _, tail = name.partition(":")
        if head in families:
            return head
        kin = {"V": "U", "Q": "G"}.get(head, head[0])
        return kin + (tail[0] if tail[0] in "12" else "s")

    buffers = {"U": ub, "V": vb, "OA": oab, "OB": obb, "G": gb, "Q": pb, "DA": dab, "DB": dbb}
    arrivals, arrival_of = [], {}
    together = [
        (n, part2.at[0, pl.ds(0, 2)], [k for k in moves if k[:2] == f"S{n}" and k[3] in "nr"]) for n in (2, 3)
    ]
    together += [
        (4, x2.at[0], ("X2:0-", "X2:2+", "X2:1-", "X2:3+")),
        (5, x2.at[0], [f"X2:f{q}" for q in range(4)]),
        (6, x1.at[0], ("X1:H0-", "X1:H1+")),
        (7, x1.at[0], ("X1:f+", "X1:f-")),
        (8, stat_in, ("stat:R", "stat:L", "stat:P")),
    ]
    known = {}
    for name, (_, _, to, ref) in moves.items():
        head = name.partition(":")[0]
        key = name
        if head in buffers:
            key = arrival_group(name)
            buf, blocks = buffers[head], key[2]
            if blocks:
                ref = {16: buf.at[0], 9: buf.at[0, pl.ds(0, 3), pl.ds(0, 3)]}.get(blocks)
                ref = buf.at[0, 0, pl.ds(0, blocks)] if ref is None else ref
        else:
            for key_of, ref_of, members in together:
                if name in members:
                    key, ref = key_of, ref_of
        if key not in known:
            known[key] = len(arrivals)
            arrivals.append((ref, to))
        arrival_of[name] = known[key]
    names = list(moves)

    def start(n):
        name = names[n]
        src, dst, to, _ = moves[name]
        pltpu.make_async_remote_copy(
            src_ref=src, dst_ref=dst, send_sem=send_sems.at[family_sem[family_of(name)]],
            recv_sem=recv_sems.at[arrival_of[name]], device_id=to, device_id_type=MESH,
        ).start()

    def arrive(n):
        ref, to = arrivals[n]
        sem = recv_sems.at[n]
        pltpu.make_async_remote_copy(
            src_ref=ref, dst_ref=ref, send_sem=sem, recv_sem=sem, device_id=to, device_id_type=MESH
        ).wait_recv()

    acts = (start, arrive, lambda n: work[n]())
    for code in ORDER:
        step = functools.partial(acts[code // 1000], code % 1000)
        step()
    for name, ref in families.items():
        sem = send_sems.at[family_sem[name]]
        pltpu.make_async_remote_copy(
            src_ref=ref, dst_ref=ref, send_sem=sem, recv_sem=sem, device_id=partner, device_id_type=MESH
        ).wait_send()


def local(
    tokens, mix_gain, ffn_gain, u_weight, u_scale, v_weight, v_scale, v_gain, spatial_weight, spatial_bias,
    out_weight, out_scale, gate_weight, gate_scale, up_weight, up_scale, down_weight, down_scale,
):
    rows, width = tokens.shape
    row = lambda a: a.reshape(1, -1)
    bias = spatial_bias.reshape(spatial_bias.shape[0], 1, BLK)
    depth = u_weight.shape[0]
    ff = gate_weight.shape[1]
    mix_cols = u_weight.shape[1]
    out_cols = out_weight.shape[1]
    vm = pltpu.VMEM
    on_chip = pl.BlockSpec(memory_space=pltpu.VMEM)
    inputs = (
        tokens, row(mix_gain), u_weight, row(u_scale), v_weight, row(v_scale), out_weight, row(out_scale), row(v_gain),
        gate_weight, gate_scale, up_weight, up_scale, down_weight, row(down_scale), spatial_weight, bias, row(ffn_gain),
    )
    in_hbm = pl.BlockSpec(memory_space=pltpu.HBM)
    scratch = [vm(a.shape, a.dtype) for a in inputs] + [
        vm((2, 4, 4, depth, mix_cols), BF16), vm((2, 4, 4, depth, mix_cols), BF16),
        vm((2, 4, 4, mix_cols // 2, out_cols), BF16), vm((2, 4, 4, mix_cols // 2, out_cols), BF16),
        vm((2, 4, 4, depth, ff), BF16), vm((2, 4, 4, depth, ff), BF16),
        vm((2, 4, 4, ff // 2, out_cols), BF16), vm((2, 4, 4, ff // 2, out_cols), BF16),
        vm((4, rows, width), BF16), vm((4, rows, width), BF16),
        vm((4, rows, 2 * mix_cols), BF16), vm((4, rows, 2 * mix_cols), BF16), vm((4, rows, 2 * mix_cols), BF16),
        vm((2, 2 * rows, 2 * ff), BF16),
        vm((4, rows, width), BF16), vm((2, 4, rows, width // 2), BF16),
        vm((rows, width), BF16), vm((2, rows, width // 2), BF16),
        vm((rows, width), BF16), vm((rows, width), BF16),
        vm((2, rows, width // 2), BF16), vm((2, rows, width // 2), BF16),
        vm((rows, width), BF16),
        vm((4, 8, BLK), F32), vm((3, 4, 8, BLK), F32), vm((2, 8, mix_cols), F32),
        pltpu.SemaphoreType.DMA((len(inputs),)),
        pltpu.SemaphoreType.DMA((N_FAMILIES,)),
        pltpu.SemaphoreType.DMA((N_ARRIVALS,)),
    ]
    return pl.pallas_call(
        layer_kernel,
        out_shape=jax.ShapeDtypeStruct(tokens.shape, BF16),
        in_specs=[in_hbm] * len(inputs),
        out_specs=on_chip,
        scratch_shapes=scratch,
        compiler_params=pltpu.CompilerParams(
            collective_id=0, has_side_effects=True, vmem_limit_bytes=60 * 1024 * 1024
        ),
    )(*inputs)


def solution(mesh):
    both = ("fs", "tp")
    in_specs = (
        P(both, None), P(), P(),
        P("fs", "tp"), P("tp"), P("fs", "tp"), P("tp"), P("tp"),
        P(), P(),
        P("tp", "fs"), P("fs"),
        P("fs", "tp"), P("tp"), P("fs", "tp"), P("tp"),
        P("tp", "fs"), P("fs"),
    )
    return jax.shard_map(local, mesh=mesh, in_specs=in_specs, out_specs=P(both, None), check_vma=False)
```

```python
import functools

import jax
import jax.numpy as jnp
from jax import lax
from jax.experimental import pallas as pl
from jax.experimental.pallas import tpu as pltpu
from jax.sharding import PartitionSpec as P

MESH = pl.DeviceIdType.MESH
F32 = jnp.float32
BF16 = jnp.bfloat16
A = 2048
BLK = 128
LEFT, RIGHT, OPP, OWN = 0, 1, 2, 3


def rms_rows(widened, norm_gain):
    factor = lax.rsqrt(jnp.mean(widened * widened, axis=1, keepdims=True) + 1e-06)
    return (widened * factor * norm_gain).astype(BF16)


def gelu(x):
    return 0.5 * x * (1.0 + jnp.tanh(0.7978845608028654 * (x + 0.044715 * (x * x * x))))


def silu(x):
    return 0.5 * x * (1.0 + jnp.tanh(0.5 * x))


ORDER = (
    184, 187, 185, 186, 235, 0, 1, 20, 21, 4, 5, 24,
    25, 2000, 136, 168, 1133, 44, 45, 64, 65, 40, 41, 60,
    61, 1000, 2, 6, 7, 1001, 3, 8, 9, 1011, 22, 26,
    27, 1012, 23, 28, 29, 1003, 12, 1014, 32, 1025, 1036, 1022,
    47, 1023, 43, 49, 1033, 67, 1034, 1102, 188, 42, 62, 63,
    52, 72, 69, 1104, 189, 1002, 16, 10, 11, 1005, 13, 1004,
    1016, 33, 1015, 1007, 14, 66, 1013, 36, 30, 31, 1018, 34,
    1026, 1037, 46, 1029, 54, 1040, 74, 48, 68, 1024, 56, 51,
    1035, 76, 71, 50, 70, 1103, 1008, 18, 15, 1006, 17, 1019,
    38, 35, 1038, 73, 1027, 53, 1030, 58, 55, 1017, 37, 1041,
    78, 75, 1028, 57, 1039, 77, 80, 81, 100, 101, 1009, 19,
    84, 85, 104, 105, 1105, 1020, 39, 1010, 1021, 2001, 2002, 233,
    234, 232, 1031, 59, 1042, 79, 120, 121, 152, 153, 1032, 1043,
    1044, 82, 86, 87, 1055, 107, 1056, 1045, 106, 1132, 2004, 2006,
    204, 205, 206, 207, 83, 102, 103, 2003, 2005, 202, 203, 1047,
    1058, 1066, 92, 112, 89, 109, 140, 1084, 172, 1085, 176, 1067,
    144, 1114, 1116, 2017, 208, 2019, 210, 1049, 93, 108, 1048, 1059,
    1115, 155, 1117, 2018, 209, 123, 2020, 211, 1057, 116, 111, 1060,
    1046, 96, 91, 113, 88, 1051, 94, 1062, 114, 1112, 1113, 1118,
    90, 110, 1120, 2029, 190, 191, 2031, 195, 194, 1052, 98, 95,
    1063, 118, 115, 1119, 1121, 2030, 192, 193, 2032, 197, 196, 122,
    154, 1106, 198, 124, 125, 156, 157, 126, 127, 158, 159, 1109,
    200, 1050, 97, 1061, 117, 1068, 148, 128, 129, 160, 161, 1086,
    180, 1053, 99, 1064, 119, 1108, 199, 1069, 137, 132, 131, 162,
    163, 1070, 138, 1087, 169, 1088, 170, 1107, 164, 130, 1110, 201,
    1071, 141, 1072, 142, 1089, 173, 1090, 174, 1054, 133, 165, 1073,
    145, 1074, 146, 134, 1091, 177, 1092, 178, 166, 1065, 2007, 2008,
    2009, 1076, 150, 135, 1077, 139, 1093, 181, 1094, 182, 167, 1111,
    2010, 1081, 1099, 2011, 1075, 149, 1095, 171, 2012, 1079, 147, 1097,
    179, 1078, 143, 1096, 175, 2014, 214, 215, 216, 217, 2013, 212,
    213, 1101, 1083, 1080, 151, 1098, 183, 1123, 1125, 2021, 218, 2023,
    220, 1082, 1100, 2016, 224, 225, 226, 227, 2015, 222, 223, 1124,
    1126, 2022, 219, 2024, 221, 1128, 1130, 2025, 228, 2027, 230, 1129,
    1131, 2026, 229, 2028, 231, 1122, 2033, 1127, 2034,
)
N_FAMILIES, N_ARRIVALS = 19, 134


COLUMNS = (
    ((0, 0), (0, -1), (0, 1), (-1, 0), (1, 0), (-1, -1), (1, 1), (-1, 1)),
    ((1, -1), (2, 0), (0, 2), (2, 1), (1, 2), (2, -1), (-1, 2), (2, 2)),
)
OFFSETS = {"o": 0, "L": -1, "R": 1, "P": 2}


def weight_transfers(name, buf, x_first, place):
    x, y, z, c = place
    low, high = pl.ds(0, buf.shape[3] // 2), pl.ds(buf.shape[3] // 2, buf.shape[3] // 2)

    def at(value, step):
        return lax.rem(value + step + 4, 4)

    def block(a, b, rows=None):
        ref = buf.at[c, at(z, b), at(x, a)] if x_first else buf.at[c, at(z, a), at(x, b)]
        return ref if rows is None else ref.at[rows]

    def group(b, core=None):
        core = c if core is None else core
        return buf.at[core, at(z, b)] if x_first else buf.at[core, :, at(x, b)]

    def device(first, step):
        along_x = first == x_first
        return (z * 4 + at(x, step), y * 2 + c) if along_x else (at(z, step) * 4 + x, y * 2 + c)

    found = {}
    for sign, step in (("+", 1), ("-", -1)):
        rows = low if step == 1 else high
        found["1" + sign] = (block(0, 0), device(True, step), block(-step, 0))
        found["1f" + sign] = (block(-step, 0, rows), device(True, step), block(2, 0, rows))
        far = device(False, step)
        for kind, a in OFFSETS.items():
            found["2" + kind + sign] = (block(a, 0), far, block(a, -step))
            found["2f" + kind + sign] = (block(a, -step), far, block(a, 2))
    partner = (z * 4 + x, y * 2 + 1 - c)
    parts = {"d0": 0, "d-": -1, "d+": 1, "d2": 2}
    for kind, a in OFFSETS.items():
        for mark, b in (("o", 0), ("-", -1), ("+", 1), ("2", 2)):
            other = buf.at[1 - c, at(z, b), at(x, a)] if x_first else buf.at[1 - c, at(z, a), at(x, b)]
            found["e" + kind + mark] = (block(a, b), partner, other)
    for key, b in parts.items():
        found[key] = (group(b), partner, group(b, core=1 - c))
    shared = list(parts) if name[0] != "D" else ["e" + kind + mark for kind in OFFSETS for mark in "o-+2"]
    used = ["1+", "1-", "1f+", "1f-"] + ["2" + kind + sign for kind in OFFSETS for sign in "+-"]
    used += ["2fo+", "2fL+", "2fR-", "2fP-"] + shared
    return {name + ":" + key: (found[key][0],) + found[key] for key in used}


def arrival_group(name):
    head, _, key = name.partition(":")
    if key[:2] == "1f":
        return head, "1f", 1
    if key[0] == "e":
        early = key[1] != "P" and key[2] != "2"
        return (head, "ea", 9) if early else (head, "eb", 4) if key[2] == "2" else (head, "ec", 3)
    if head[0] != "D":
        if key[0] == "d":
            return head, "d", 16
        if key[:2] == "2f":
            return head, "2f", 4
        if key in ("2R+", "2P+"):
            return head, "2a", 2
        if key in ("2o-", "2L-"):
            return head, "2b", 2
    return head, key, 0


def layer_kernel(
    *refs,
):
    held_in_hbm, out_ref, held, refs = refs[:18], refs[18], refs[19:37], refs[37:]
    tok, mix_gain, u32, u_scale, v32, v_scale, o32, o_scale, v_gain, g32, g_scale, p32, p_scale, d32, d_scale, *rest = held
    spatial, bias, ffn_gain = rest
    (
        ub, vb, oab, obb, gb, pb, dab, dbb,
        x1, x2, u_val, v_val, gated, hid, part1, part2, relay1, relay2, fl1, fr1, fl2, fr2, res,
        stat, stat_in, vg,
        load_sems, send_sems, recv_sems,
    ) = refs
    fs = lax.axis_index("fs")
    tp = lax.axis_index("tp")
    z, x = fs // 4, lax.rem(fs, 4)
    y, c = tp // 2, lax.rem(tp, 2)
    partner = (fs, y * 2 + 1 - c)
    y_right = (fs, lax.rem(y + 1, 4) * 2 + c)
    y_left = (fs, lax.rem(y + 3, 4) * 2 + c)
    y_opp = (fs, lax.rem(y + 2, 4) * 2 + c)

    loads = []
    for n, (src, dst) in enumerate(zip(held_in_hbm, held)):
        copy = pltpu.make_async_copy(src, dst, load_sems.at[n])
        copy.start()
        loads.append((n, copy))

    barrier = pltpu.get_barrier_semaphore()
    plane = [
        (z * 4 + lax.rem(x + 1, 4), tp),
        (z * 4 + lax.rem(x + 3, 4), tp),
        (lax.rem(z + 1, 4) * 4 + x, tp),
        (lax.rem(z + 3, 4) * 4 + x, tp),
    ]
    peers = [partner, y_right, y_left, y_opp] + plane
    for peer in peers:
        pl.semaphore_signal(barrier, inc=1, device_id=peer, device_id_type=MESH)

    def ready(last):
        while loads[0][0] <= last:
            loads.pop(0)[1].wait()
            if not loads:
                break

    ready(3 + 2)
    ub[c, z, x] = (u32[...] * u_scale[...]).astype(BF16)
    vb[c, z, x] = (v32[...] * v_scale[...]).astype(BF16)
    x1[OWN] = rms_rows(tok[...].astype(F32), mix_gain[...])
    ready(8)
    half = o32.shape[0] // 2
    oab[c, z, x] = (o32[:half] * o_scale[...]).astype(BF16)
    obb[c, z, x] = (o32[half:] * o_scale[...]).astype(BF16)
    vg[c] = jnp.broadcast_to(v_gain[...], vg.shape[1:])

    pl.semaphore_wait(barrier, len(peers))


    moves = {}
    for n, (name, buf) in enumerate(
        (("U", ub), ("V", vb), ("OA", oab), ("OB", obb), ("G", gb), ("Q", pb), ("DA", dab), ("DB", dbb))
    ):
        moves.update(weight_transfers(name, buf, n % 2 == 0, (x, y, z, c)))

    H0, H1 = pl.ds(0, 64), pl.ds(64, 64)
    Q = [pl.ds(32 * q, 32) for q in range(4)]

    def rows_move(buf, to_right, rows):
        to = LEFT if to_right else RIGHT
        return (buf.at[OWN, rows], buf.at[to, rows], y_right if to_right else y_left, buf.at[to, rows])

    def pass_on(buf, to_right, rows):
        kept = LEFT if to_right else RIGHT
        return (buf.at[kept, rows], buf.at[OPP, rows], y_right if to_right else y_left, buf.at[OPP, rows])

    moves["X1:H0+"] = rows_move(x1, True, H0)
    moves["X1:H0-"] = rows_move(x1, False, H0)
    moves["X1:H1+"] = rows_move(x1, True, H1)
    moves["X1:H1-"] = rows_move(x1, False, H1)
    moves["X1:f+"] = pass_on(x1, True, H0)
    moves["X1:f-"] = pass_on(x1, False, H1)
    for q in range(4):
        moves[f"X2:{q}+"] = rows_move(x2, True, Q[q])
        moves[f"X2:{q}-"] = rows_move(x2, False, Q[q])
    for q in range(4):
        moves[f"X2:f{q}"] = pass_on(x2, q < 2, Q[q])
    for key, part, relay, fl, fr in (
        ("S1", part1, relay1, fl1, fr1),
        ("S2", part2.at[0], relay2.at[0], fl2.at[0], fr2.at[0]),
        ("S3", part2.at[1], relay2.at[1], fl2.at[1], fr2.at[1]),
    ):
        moves[f"{key}:n+"] = (part.at[RIGHT, H1], fl.at[H1], y_right, fl.at[H1])
        moves[f"{key}:n-"] = (part.at[LEFT, H0], fr.at[H0], y_left, fr.at[H0])
        for q in range(4):
            to = y_right if q < 2 else y_left
            moves[f"{key}:o{q}"] = (part.at[OPP, Q[q]], relay.at[Q[q]], to, relay.at[Q[q]])
        for q in range(4):
            near, into, to = (RIGHT, fl, y_right) if q < 2 else (LEFT, fr, y_left)
            moves[f"{key}:r{q}"] = (part.at[near, Q[q]], into.at[Q[q]], to, into.at[Q[q]])
    moves["stat:R"] = (stat, stat_in.at[0], y_right, stat_in.at[0])
    moves["stat:L"] = (stat, stat_in.at[1], y_left, stat_in.at[1])
    moves["stat:P"] = (stat, stat_in.at[2], y_opp, stat_in.at[2])
    moves["vg"] = (vg.at[c], vg.at[c], partner, vg.at[1 - c])

    slot_chip = [lax.rem(y + 3, 4), lax.rem(y + 1, 4), lax.rem(y + 2, 4), y]
    row_ids = lax.broadcasted_iota(jnp.int32, (BLK, BLK), 0)
    col_ids = lax.broadcasted_iota(jnp.int32, (BLK, BLK), 1)
    eye = row_ids == col_ids

    def project_mixer(first):
        rows = x1[first : first + 2].reshape(2 * BLK, -1)
        sums = squares = 0.0
        for core in range(2):
            cols = slice(core * 256, core * 256 + 256)
            u = gelu(jnp.dot(rows, ub[core].reshape(A, 256), preferred_element_type=F32))
            v = gelu(jnp.dot(rows, vb[core].reshape(A, 256), preferred_element_type=F32)).astype(BF16)
            u_val[first : first + 2, :, cols] = u.astype(BF16).reshape(2, BLK, 256)
            v_val[first : first + 2, :, cols] = v.reshape(2, BLK, 256)
            wide = v.astype(F32)
            sums = sums + jnp.sum(wide, axis=1, keepdims=True)
            squares = squares + jnp.sum(wide * wide, axis=1, keepdims=True)
        for k in range(2):
            for row, column in ((0, sums), (1, squares)):
                piece = column[k * BLK : (k + 1) * BLK]
                stat[slot_chip[first + k], row : row + 1, :] = jnp.sum(
                    jnp.where(eye, piece, 0.0), axis=0, keepdims=True
                )

    def mixing_rows(core):
        masked = jnp.where(col_ids <= row_ids, spatial[2 * y + core].astype(F32), 0.0)
        offset = jnp.sum(jnp.where(eye, bias[2 * y + core], 0.0), axis=1, keepdims=True)
        return masked, offset

    def mix(slot):
        chip = slot_chip[slot]
        total = stat[chip] + stat_in[0, chip] + stat_in[1, chip] + stat_in[2, chip]
        average = total[0:1] * (1.0 / A)
        spread = total[1:2] * (1.0 / A) - average * average
        factor = lax.rsqrt(spread + 1e-05)
        for core in range(2):
            cols = slice(core * 256, core * 256 + 256)
            masked, offset = mixing_rows(core)
            scaled = (masked * factor).astype(BF16)
            shift = jnp.sum(scaled.astype(F32) * average, axis=1, keepdims=True)
            mixed = jnp.dot(scaled, v_val[slot, :, cols], preferred_element_type=F32)
            mixed = (mixed - shift) * vg[core, 0:1, :] + offset
            gated[slot, :, cols] = (u_val[slot, :, cols].astype(F32) * mixed).astype(BF16)

    def project_out(first):
        rows = gated[first : first + 2].reshape(2 * BLK, -1)
        for j in range(8):
            fz, fx = j // 2, (j % 2) * 2
            matrix = jnp.concatenate(
                [
                    jnp.concatenate([buf[core, fz, fx + k] for core in range(2) for buf in (oab, obb)], axis=0)
                    for k in range(2)
                ],
                axis=1,
            )
            total = jnp.dot(rows, matrix, preferred_element_type=F32)
            part1[first : first + 2, :, j * 256 : j * 256 + 256] = total.astype(BF16).reshape(2, BLK, 256)

    def project_ffn(first, part):
        rows = x2[first : first + 2].reshape(2 * BLK, -1)
        for n in (2 * part, 2 * part + 1):
            core, j = n // 3, n % 3
            cols = slice(j * 256, j * 256 + 256)
            gate = jnp.dot(rows, gb[core, :, :, :, cols].reshape(A, 256), preferred_element_type=F32)
            up = jnp.dot(rows, pb[core, :, :, :, cols].reshape(A, 256), preferred_element_type=F32)
            hid[first // 2, :, n * 256 : n * 256 + 256] = (silu(gate) * up).astype(BF16)

    def place_of(dz, dx):
        return lax.rem(z + dz + 4, 4), lax.rem(x + dx + 4, 4)

    def project_down(first, part):
        rows = hid[first // 2]
        for j in range(0, 8, 2):
            pair = []
            for dz, dx in COLUMNS[part][j : j + 2]:
                fz, fx = place_of(dz, dx)
                pair.append(
                    jnp.concatenate([buf[core, fz, fx] for core in range(2) for buf in (dab, dbb)], axis=0)
                )
            total = jnp.dot(rows, jnp.concatenate(pair, axis=1), preferred_element_type=F32)
            cols = slice(j * BLK, j * BLK + 256)
            part2[part, first : first + 2, :, cols] = total.astype(BF16).reshape(2, BLK, 256)

    def add_relayed(part, relay, q):
        near = RIGHT if q < 2 else LEFT
        part[near, Q[q]] = (part[near, Q[q]].astype(F32) + relay[Q[q]].astype(F32)).astype(BF16)

    def second_norm(q):
        total = tok[Q[q]].astype(F32) + part1[OWN, Q[q]].astype(F32)
        residual = (total + fl1[Q[q]].astype(F32) + fr1[Q[q]].astype(F32)).astype(BF16)
        res[Q[q]] = residual
        x2[OWN, Q[q]] = rms_rows(residual.astype(F32), ffn_gain[...])

    def finish(part):
        for j, (dz, dx) in enumerate(COLUMNS[part]):
            fz, fx = place_of(dz, dx)
            cols = pl.ds(pl.multiple_of((fz * 4 + fx) * BLK, BLK), BLK)
            held = slice(j * BLK, j * BLK + BLK)
            total = res[:, cols].astype(F32) + part2[part, OWN, :, held].astype(F32)
            total = total + fl2[part, :, held].astype(F32) + fr2[part, :, held].astype(F32)
            out_ref[:, cols] = total.astype(BF16)

    def convert_rest():
        ready(14)
        gb[c, z, x] = (g32[...] * g_scale[...].reshape(1, -1)).astype(BF16)
        pb[c, z, x] = (p32[...] * p_scale[...].reshape(1, -1)).astype(BF16)
        half = d32.shape[0] // 2
        dab[c, z, x] = (d32[:half] * d_scale[...]).astype(BF16)
        dbb[c, z, x] = (d32[half:] * d_scale[...]).astype(BF16)
        stat[...] = jnp.zeros_like(stat)
        ready(17)

    halves = (LEFT, OPP)
    work = [convert_rest]
    work += [functools.partial(project_mixer, first) for first in halves]
    work += [lambda: (mix(LEFT), mix(RIGHT)), lambda: (mix(OPP), mix(OWN))]
    work += [functools.partial(project_out, first) for first in halves]
    work += [functools.partial(project_ffn, first, n) for first in halves for n in range(3)]
    work += [functools.partial(project_down, first, part) for part in range(2) for first in halves]
    for part, relay in ((part1, relay1), (part2.at[0], relay2.at[0]), (part2.at[1], relay2.at[1])):
        work += [functools.partial(add_relayed, part, relay, q) for q in range(4)]
    work += [functools.partial(second_norm, q) for q in range(4)]
    work += [functools.partial(finish, part) for part in range(2)]

    families = {}
    for n, buf in (("U", ub), ("O", oab), ("G", gb), ("D", dab)):
        families[n + "1"] = buf.at[:, 0, pl.ds(0, 3)]
        families[n + "2"] = buf.at[:, pl.ds(0, 3)]
        families[n + "s"] = buf
    families["X1"], families["X2"], families["S1"] = x1.at[pl.ds(0, 3)], x2.at[pl.ds(0, 3)], part1.at[pl.ds(0, 3)]
    families["S2"], families["S3"] = part2.at[0, pl.ds(0, 3)], part2.at[1, pl.ds(0, 3)]
    families["stat"], families["vg"] = stat_in, vg.at[0]
    family_sem = {name: n for n, name in enumerate(families)}

    def family_of(name):
        head, _, tail = name.partition(":")
        if head in families:
            return head
        kin = {"V": "U", "Q": "G"}.get(head, head[0])
        return kin + (tail[0] if tail[0] in "12" else "s")

    buffers = {"U": ub, "V": vb, "OA": oab, "OB": obb, "G": gb, "Q": pb, "DA": dab, "DB": dbb}
    arrivals, arrival_of = [], {}
    together = [
        (n, part2.at[0, pl.ds(0, 2)], [k for k in moves if k[:2] == f"S{n}" and k[3] in "nr"]) for n in (2, 3)
    ]
    together += [
        (4, x2.at[0], ("X2:0-", "X2:2+", "X2:1-", "X2:3+")),
        (5, x2.at[0], [f"X2:f{q}" for q in range(4)]),
        (6, x1.at[0], ("X1:H0-", "X1:H1+")),
        (7, x1.at[0], ("X1:f+", "X1:f-")),
        (8, stat_in, ("stat:R", "stat:L", "stat:P")),
    ]
    known = {}
    for name, (_, _, to, ref) in moves.items():
        head = name.partition(":")[0]
        key = name
        if head in buffers:
            key = arrival_group(name)
            buf, blocks = buffers[head], key[2]
            if blocks:
                ref = {16: buf.at[0], 9: buf.at[0, pl.ds(0, 3), pl.ds(0, 3)]}.get(blocks)
                ref = buf.at[0, 0, pl.ds(0, blocks)] if ref is None else ref
        else:
            for key_of, ref_of, members in together:
                if name in members:
                    key, ref = key_of, ref_of
        if key not in known:
            known[key] = len(arrivals)
            arrivals.append((ref, to))
        arrival_of[name] = known[key]
    names = list(moves)

    def start(n):
        name = names[n]
        src, dst, to, _ = moves[name]
        pltpu.make_async_remote_copy(
            src_ref=src, dst_ref=dst, send_sem=send_sems.at[family_sem[family_of(name)]],
            recv_sem=recv_sems.at[arrival_of[name]], device_id=to, device_id_type=MESH,
        ).start()

    def arrive(n):
        ref, to = arrivals[n]
        sem = recv_sems.at[n]
        pltpu.make_async_remote_copy(
            src_ref=ref, dst_ref=ref, send_sem=sem, recv_sem=sem, device_id=to, device_id_type=MESH
        ).wait_recv()

    acts = (start, arrive, lambda n: work[n]())
    for code in ORDER:
        step = functools.partial(acts[code // 1000], code % 1000)
        step()
    for name, ref in families.items():
        sem = send_sems.at[family_sem[name]]
        pltpu.make_async_remote_copy(
            src_ref=ref, dst_ref=ref, send_sem=sem, recv_sem=sem, device_id=partner, device_id_type=MESH
        ).wait_send()


def local(
    tokens, mix_gain, ffn_gain, u_weight, u_scale, v_weight, v_scale, v_gain, spatial_weight, spatial_bias,
    out_weight, out_scale, gate_weight, gate_scale, up_weight, up_scale, down_weight, down_scale,
):
    rows, width = tokens.shape
    row = lambda a: a.reshape(1, -1)
    bias = spatial_bias.reshape(spatial_bias.shape[0], 1, BLK)
    depth = u_weight.shape[0]
    ff = gate_weight.shape[1]
    mix_cols = u_weight.shape[1]
    out_cols = out_weight.shape[1]
    vm = pltpu.VMEM
    on_chip = pl.BlockSpec(memory_space=pltpu.VMEM)
    inputs = (
        tokens, row(mix_gain), u_weight, row(u_scale), v_weight, row(v_scale), out_weight, row(out_scale), row(v_gain),
        gate_weight, gate_scale, up_weight, up_scale, down_weight, row(down_scale), spatial_weight, bias, row(ffn_gain),
    )
    in_hbm = pl.BlockSpec(memory_space=pltpu.HBM)
    scratch = [vm(a.shape, a.dtype) for a in inputs] + [
        vm((2, 4, 4, depth, mix_cols), BF16), vm((2, 4, 4, depth, mix_cols), BF16),
        vm((2, 4, 4, mix_cols // 2, out_cols), BF16), vm((2, 4, 4, mix_cols // 2, out_cols), BF16),
        vm((2, 4, 4, depth, ff), BF16), vm((2, 4, 4, depth, ff), BF16),
        vm((2, 4, 4, ff // 2, out_cols), BF16), vm((2, 4, 4, ff // 2, out_cols), BF16),
        vm((4, rows, width), BF16), vm((4, rows, width), BF16),
        vm((4, rows, 2 * mix_cols), BF16), vm((4, rows, 2 * mix_cols), BF16), vm((4, rows, 2 * mix_cols), BF16),
        vm((2, 2 * rows, 2 * ff), BF16),
        vm((4, rows, width), BF16), vm((2, 4, rows, width // 2), BF16),
        vm((rows, width), BF16), vm((2, rows, width // 2), BF16),
        vm((rows, width), BF16), vm((rows, width), BF16),
        vm((2, rows, width // 2), BF16), vm((2, rows, width // 2), BF16),
        vm((rows, width), BF16),
        vm((4, 8, BLK), F32), vm((3, 4, 8, BLK), F32), vm((2, 8, mix_cols), F32),
        pltpu.SemaphoreType.DMA((len(inputs),)),
        pltpu.SemaphoreType.DMA((N_FAMILIES,)),
        pltpu.SemaphoreType.DMA((N_ARRIVALS,)),
    ]
    return pl.pallas_call(
        layer_kernel,
        out_shape=jax.ShapeDtypeStruct(tokens.shape, BF16),
        in_specs=[in_hbm] * len(inputs),
        out_specs=on_chip,
        scratch_shapes=scratch,
        compiler_params=pltpu.CompilerParams(
            collective_id=0, has_side_effects=True, vmem_limit_bytes=60 * 1024 * 1024
        ),
    )(*inputs)


def solution(mesh):
    both = ("fs", "tp")
    in_specs = (
        P(both, None), P(), P(),
        P("fs", "tp"), P("tp"), P("fs", "tp"), P("tp"), P("tp"),
        P(), P(),
        P("tp", "fs"), P("fs"),
        P("fs", "tp"), P("tp"), P("fs", "tp"), P("tp"),
        P("tp", "fs"), P("fs"),
    )
    return jax.shard_map(local, mesh=mesh, in_specs=in_specs, out_specs=P(both, None), check_vma=False)
```
